32 devices in a mesh: sp: 8 (over z, x), tp: 4 (over y, core).
Axes of the slice: x: 2, y: 2, z: 4, core: 2. Of those that a mesh axis runs over, the one named last changes fastest.
Arguments:
- incoming_residual_stream: bfloat16 [4096, 2048], P(('sp', 'tp')), may hold values from -6 to 6
- result_valve: bfloat16 [4096, 2048], P('sp', 'tp'), may hold values from -6 to 6
- channel_feed_matrix: bfloat16 [4096, 2048], P('sp', 'tp'), may hold values from -6 to 6
- memory_feed_matrix: bfloat16 [4096, 512], P('sp', 'tp'), may hold values from -6 to 6
- memory_query_matrix: bfloat16 [4096, 512], P('sp', 'tp'), may hold values from -6 to 6
- unsoftened_deltas: float32 [4096, 32], P('sp', 'tp'), may hold values from -2.7 to 2.7
- delta_offset: float32 [32], P('tp'), may hold values from -4.5 to -3.5
- channel_fading_speed: float32 [32], P('tp'), as said below
- extra_log_fading: float32 [4096, 32], P('sp', 'tp'), may hold values from -0.7 to 0
- bypass_factor: float32 [32], P('tp'), may hold values from 0.1 to 1.9
- channel_feed_kernel: bfloat16 [4, 2048], P(None, 'tp'), may hold values from -3 to 3
- memory_feed_kernel: bfloat16 [4, 512], P(None, 'tp'), may hold values from -3 to 3
- memory_query_kernel: bfloat16 [4, 512], P(None, 'tp'), may hold values from -3 to 3
- cluster_scaling_vector: float32 [2048], P('tp'), may hold values from 0.1 to 1.9
- mixer_result_matrix: bfloat16 [2048, 2048], P('tp'), may hold values from -0.125 to 0.125
- initial_scaling_vector: float32 [2048], replicated, may hold values from 0.1 to 1.9
- valve_matrix: bfloat16 [2048, 5632], P('sp', 'tp'), may hold values from -0.125 to 0.125
- widen_matrix: bfloat16 [2048, 5632], P('sp', 'tp'), may hold values from -0.125 to 0.125
- shrink_matrix: bfloat16 [5632, 2048], P('tp', 'sp'), may hold values from -0.078125 to 0.078125
- valve_filter_kernel: bfloat16 [3, 5632], P(None, 'tp'), may hold values from -3.5 to 3.5
- widen_filter_kernel: bfloat16 [3, 5632], P(None, 'tp'), may hold values from -3.5 to 3.5
- latter_scaling_vector: float32 [2048], replicated, may hold values from 0.1 to 1.9
Outputs:
- layer_out: bfloat16 [4096, 2048], P(('sp', 'tp'))
The draws below stay inside these ranges and needn't reach their ends.
Inputs may be any that keep to these rules, and one draw needn't show every extreme that they name: `channel_fading_speed`: positive.
All inputs are finite; a program needn't handle non-finite values.
Results may differ from the reference program's by a relative error of at most 0.02.
Values may be sent and summed in bfloat16 or wider, within the bound.
A program may use at most 128 MiB of HBM per device.

```python
import math
import jax
import jax.numpy as jnp
from jax import lax

D = 2048
HEADS = 32
HEAD_DIM = 64
GROUPS = 4
STATE = 128
FF = 5632
CONV = 4
FCONV = 3
BLOCK = 128
TOK_DEV = 512
INNER = 2048
TOKENS = 4096
N_TP = 4


def draw_unsoftened_deltas(key, part):
    noise_key = jax.random.fold_in(key, 11)
    block_key = jax.random.fold_in(key, 12)
    centred_part = jnp.clip(0.5 * jax.random.normal(noise_key, (TOKENS, HEADS), jnp.float32), -2.0, 2.0)
    shifts = jax.random.uniform(block_key, (TOKENS // TOK_DEV, 1), jnp.float32, -0.7, 0.7)
    return centred_part + jnp.repeat(shifts, TOK_DEV, axis=0)


def draw_channel_fading_speed(key, part):
    slow_share = 0.5
    slow_mask = jax.random.uniform(jax.random.fold_in(key, 21), (HEADS,), jnp.float32) < slow_share
    fast_rate = jnp.exp(jax.random.uniform(jax.random.fold_in(key, 22), (HEADS,), jnp.float32, 0.0, math.log(4.0)))
    slow_rate = jax.random.uniform(jax.random.fold_in(key, 23), (HEADS,), jnp.float32, 10.0, 30.0) / TOKENS
    return jnp.where(slow_mask, slow_rate, fast_rate)


def draw_extra_log_fading(key, part):
    hits = jax.random.uniform(jax.random.fold_in(key, 31), (TOKENS, HEADS), jnp.float32) < 4.0 / TOKENS
    drops = jnp.log(jax.random.uniform(jax.random.fold_in(key, 32), (TOKENS, HEADS), jnp.float32, 0.5, 0.8))
    return jnp.where(hits, drops, 0.0)


def block_levels(key, dims, cuts, least, largest):
    level = 1.0
    for axis_at, shards_of in cuts:
        heights = jax.random.uniform(jax.random.fold_in(jax.random.fold_in(key, 6), axis_at), (shards_of,), jnp.float32, least / len(cuts), largest / len(cuts))
        level = level * jnp.repeat(jnp.exp(heights), dims[axis_at] // shards_of).reshape((-1,) + (1,) * (len(dims) - 1 - axis_at))
    return level


def noise(rng, dims, scale, limit, cuts=(), held_as=jnp.bfloat16):
    result = jax.random.normal(rng, dims, jnp.float32) * scale
    if len(cuts) > 0:
        result = block_levels(rng, dims, cuts, -0.22, 0.18) * result
    return jnp.clip(result, min=-limit, max=limit).astype(held_as)


def setup_inputs(seed: int = 0) -> dict:
    keys = jax.random.split(jax.random.key(seed), 23)
    incoming_residual_stream = noise(keys[0], (TOKENS, D), 1.0, 6.0, ((0, 32),))
    result_valve = noise(keys[1], (TOKENS, INNER), 1.0, 6.0, ((0, 8), (1, 4)))
    channel_feed_matrix = noise(keys[2], (TOKENS, INNER), 1.0, 6.0, ((0, 8), (1, 4)))
    memory_feed_matrix = noise(keys[3], (TOKENS, GROUPS * STATE), 1.0, 6.0, ((0, 8), (1, 4)))
    memory_query_matrix = noise(keys[4], (TOKENS, GROUPS * STATE), 1.0, 6.0, ((0, 8), (1, 4)))
    unsoftened_deltas = draw_unsoftened_deltas(jax.random.fold_in(keys[22], 71), 0)
    delta_offset = jnp.clip(-4.5 + 1.0 * jax.random.uniform(keys[6], (HEADS,), jnp.float32) ** block_levels(keys[6], (HEADS,), ((0, 4),), -0.2, 0.2), -4.5, -3.5)
    channel_fading_speed = draw_channel_fading_speed(jax.random.fold_in(keys[22], 71), 0)
    extra_log_fading = draw_extra_log_fading(jax.random.fold_in(keys[22], 71), 0)
    bypass_factor = jnp.clip(1.0 + 0.18 * jax.random.normal(keys[9], (HEADS,), jnp.float32), 0.1, 1.9)
    channel_feed_kernel = noise(keys[10], (CONV, INNER), CONV ** -0.5, 3.0, ((1, 4),))
    memory_feed_kernel = noise(keys[11], (CONV, GROUPS * STATE), CONV ** -0.5, 3.0, ((1, 4),))
    memory_query_kernel = noise(keys[12], (CONV, GROUPS * STATE), CONV ** -0.5, 3.0, ((1, 4),))
    cluster_scaling_vector = jnp.clip(1.0 + 0.18 * jax.random.normal(keys[13], (INNER,), jnp.float32), 0.1, 1.9)
    mixer_result_matrix = noise(keys[14], (INNER, D), INNER ** -0.5, 0.125, ((0, 4),))
    initial_scaling_vector = jnp.clip(1.0 + 0.18 * jax.random.normal(keys[15], (D,), jnp.float32), 0.1, 1.9)
    valve_matrix = noise(keys[16], (D, FF), D ** -0.5, 0.125, ((0, 8), (1, 4)))
    widen_matrix = noise(keys[17], (D, FF), D ** -0.5, 0.125, ((0, 8), (1, 4)))
    shrink_matrix = noise(keys[18], (FF, D), FF ** -0.5, 0.078125, ((0, 4), (1, 8)))
    valve_filter_kernel = noise(keys[19], (FCONV, FF), FCONV ** -0.5, 3.5, ((1, 4),))
    widen_filter_kernel = noise(keys[20], (FCONV, FF), FCONV ** -0.5, 3.5, ((1, 4),))
    latter_scaling_vector = jnp.clip(1.0 + 0.18 * jax.random.normal(keys[21], (D,), jnp.float32), 0.1, 1.9)
    return {"incoming_residual_stream": incoming_residual_stream, "result_valve": result_valve, "channel_feed_matrix": channel_feed_matrix, "memory_feed_matrix": memory_feed_matrix, "memory_query_matrix": memory_query_matrix, "unsoftened_deltas": unsoftened_deltas, "delta_offset": delta_offset, "channel_fading_speed": channel_fading_speed, "extra_log_fading": extra_log_fading, "bypass_factor": bypass_factor, "channel_feed_kernel": channel_feed_kernel, "memory_feed_kernel": memory_feed_kernel, "memory_query_kernel": memory_query_kernel, "cluster_scaling_vector": cluster_scaling_vector, "mixer_result_matrix": mixer_result_matrix, "initial_scaling_vector": initial_scaling_vector, "valve_matrix": valve_matrix, "widen_matrix": widen_matrix, "shrink_matrix": shrink_matrix, "valve_filter_kernel": valve_filter_kernel, "widen_filter_kernel": widen_filter_kernel, "latter_scaling_vector": latter_scaling_vector}


EPSILON = 1e-05
ALPHA = 2.0 ** 0.25
HIGHEST = lax.Precision.HIGHEST

def causal_conv(signal, before, tap_weights):
    tap_count = tap_weights.shape[0]
    row_count = signal.shape[0]
    padded = jnp.concatenate([before, signal], axis=0).astype(jnp.float32)
    running = jnp.zeros(signal.shape, jnp.float32)
    for tap_index in range(tap_count):
        running = running + tap_weights[tap_index].astype(jnp.float32) * padded[tap_index:tap_index + row_count]
    return running

def zero_rim(signal, tap_count):
    return jnp.zeros((tap_count - 1, signal.shape[1]), signal.dtype)

def layer_norm(values, scales):
    row_mean = lax.optimization_barrier(jnp.mean(values, axis=-1, keepdims=True))
    centred = values - row_mean
    spread = lax.optimization_barrier(jnp.mean(centred * centred, axis=-1, keepdims=True))
    return centred * lax.rsqrt(spread + EPSILON) * scales

def block_sum(activations, weights, pieces):
    slice_width = activations.shape[1] // pieces
    running = jnp.zeros((activations.shape[0], weights.shape[1]), jnp.float32)
    for piece_index in range(pieces):
        lower = piece_index * slice_width
        partial_value = jnp.dot(activations[:, lower:lower + slice_width], weights[lower:lower + slice_width], preferred_element_type=jnp.float32)
        rounded = lax.optimization_barrier(partial_value.astype(jnp.bfloat16))
        running = running + rounded.astype(jnp.float32)
    return running

def ssd_block(state_now, inputs):
    x_blk, b_blk, c_blk, decay_blk = inputs
    cum_decay = jnp.cumsum(decay_blk, axis=0)
    block_len = decay_blk.shape[0]
    causal = jnp.tril(jnp.ones((block_len, block_len), dtype=bool))
    between = cum_decay[:, None] - cum_decay[None, :]
    lag = jnp.exp(jnp.where(causal[:, :, None, None], between, -jnp.inf))
    affinity = jnp.einsum('lgn,sgn->lsg', c_blk, b_blk, precision=HIGHEST)
    mixing = affinity[..., None] * lag
    within = jnp.einsum('lsgh,sghp->lghp', mixing, x_blk, precision=HIGHEST)
    carried = jnp.einsum('lgn,ghpn->lghp', c_blk, state_now, precision=HIGHEST) * jnp.exp(cum_decay)[..., None]
    to_end = jnp.exp(cum_decay[-1] - cum_decay)
    fresh = jnp.einsum('lgn,lghp->ghpn', b_blk, x_blk * to_end[..., None], precision=HIGHEST)
    state_next = state_now * jnp.exp(cum_decay[-1])[..., None, None] + fresh
    return (state_next, within + carried)

def reference(incoming_residual_stream, result_valve, channel_feed_matrix, memory_feed_matrix, memory_query_matrix, unsoftened_deltas, delta_offset, channel_fading_speed, extra_log_fading, bypass_factor, channel_feed_kernel, memory_feed_kernel, memory_query_kernel, cluster_scaling_vector, mixer_result_matrix, initial_scaling_vector, valve_matrix, widen_matrix, shrink_matrix, valve_filter_kernel, widen_filter_kernel, latter_scaling_vector):
    group_heads = HEADS // GROUPS
    x_act = jax.nn.silu(causal_conv(channel_feed_matrix, zero_rim(channel_feed_matrix, CONV), channel_feed_kernel)).astype(jnp.bfloat16)
    b_act = jax.nn.silu(causal_conv(memory_feed_matrix, zero_rim(memory_feed_matrix, CONV), memory_feed_kernel)).astype(jnp.bfloat16)
    c_act = jax.nn.silu(causal_conv(memory_query_matrix, zero_rim(memory_query_matrix, CONV), memory_query_kernel)).astype(jnp.bfloat16)
    channel_delta_amount = jax.nn.softplus(unsoftened_deltas + delta_offset[None, :])
    log_fading_amount = extra_log_fading - channel_fading_speed[None, :] * channel_delta_amount
    block_count = TOKENS // BLOCK
    x_heads = x_act.astype(jnp.float32).reshape(TOKENS, GROUPS, group_heads, HEAD_DIM)
    x_scaled = x_heads * channel_delta_amount.reshape(TOKENS, GROUPS, group_heads)[..., None]
    x_blocks = x_scaled.reshape(block_count, BLOCK, GROUPS, group_heads, HEAD_DIM)
    b_blocks = b_act.astype(jnp.float32).reshape(block_count, BLOCK, GROUPS, STATE)
    c_blocks = c_act.astype(jnp.float32).reshape(block_count, BLOCK, GROUPS, STATE)
    decay_blocks = log_fading_amount.reshape(block_count, BLOCK, GROUPS, group_heads)
    initial = jnp.zeros((GROUPS, group_heads, HEAD_DIM, STATE), jnp.float32)
    _, mixed = lax.scan(ssd_block, initial, (x_blocks, b_blocks, c_blocks, decay_blocks))
    y_heads = mixed.reshape(TOKENS, GROUPS, group_heads, HEAD_DIM)
    y_heads = y_heads + bypass_factor.reshape(GROUPS, group_heads)[None, :, :, None] * x_heads
    gated = y_heads.reshape(TOKENS, GROUPS, INNER // GROUPS)
    gated = gated * jax.nn.silu(result_valve.astype(jnp.float32)).reshape(TOKENS, GROUPS, INNER // GROUPS)
    gated = gated * lax.rsqrt(lax.optimization_barrier(jnp.mean(gated * gated, axis=-1, keepdims=True)) + EPSILON)
    y_norm = (gated.reshape(TOKENS, INNER) * cluster_scaling_vector[None, :]).astype(jnp.bfloat16)
    mixer = block_sum(y_norm, mixer_result_matrix, N_TP)
    normed = layer_norm(ALPHA * incoming_residual_stream.astype(jnp.float32) + mixer, initial_scaling_vector).astype(jnp.bfloat16)
    gate_proj = jnp.dot(normed, valve_matrix, preferred_element_type=jnp.float32).astype(jnp.bfloat16)
    up_proj = jnp.dot(normed, widen_matrix, preferred_element_type=jnp.float32).astype(jnp.bfloat16)
    gate_conv = causal_conv(gate_proj, zero_rim(gate_proj, FCONV), valve_filter_kernel)
    up_conv = causal_conv(up_proj, zero_rim(up_proj, FCONV), widen_filter_kernel)
    hidden = (jax.nn.silu(gate_conv) * up_conv).astype(jnp.bfloat16)
    channel = block_sum(hidden, shrink_matrix, N_TP)
    return layer_norm(ALPHA * normed.astype(jnp.float32) + channel, latter_scaling_vector).astype(jnp.bfloat16)
```

```python
import functools
import jax
import jax.numpy as jnp
from jax import lax
from jax.experimental import pallas as pl
from jax.experimental.pallas import tpu as pltpu
from jax.sharding import PartitionSpec as P

HEADS = 32
HEAD_DIM = 64
GROUPS = 4
STATE = 128
CONV = 4
FCONV = 3
BLOCK = 128


EPSILON = 1e-05
ALPHA = 2.0**0.25
HIGHEST = lax.Precision.HIGHEST


def shifted(shard, axis, by):
    count = lax.axis_size(axis)
    pairs = [(i, i + by) for i in range(count) if 0 <= i + by < count]
    return lax.ppermute(shard, axis, pairs)


def entering(shard, axis, join, neutral):
    place = lax.axis_index(axis)
    gathered = jax.tree.map(
        lambda a, kind: lax.all_gather(a.astype(kind), axis), shard, (jnp.bfloat16, jnp.bfloat16)
    )
    state = jax.tree.map(lambda a, e: jnp.zeros_like(a) + jnp.asarray(e, a.dtype), shard, neutral)

    def one(lap, state):
        return join(
            state,
            jax.tree.map(
                lambda a, own: lax.dynamic_index_in_dim(a, lap, 0, False).astype(own.dtype),
                gathered,
                shard,
            ),
        )

    return lax.fori_loop(0, place, one, state)


def causal_conv(signal, before, tap_weights):
    tap_count = tap_weights.shape[0]
    row_count = signal.shape[0]
    padded = jnp.concatenate([before, signal], axis=0).astype(jnp.float32)
    running = jnp.zeros(signal.shape, jnp.float32)
    for tap_index in range(tap_count):
        running = (
            running
            + tap_weights[tap_index].astype(jnp.float32) * padded[tap_index : tap_index + row_count]
        )
    return running


def layer_norm(values, scales):
    row_mean = jnp.mean(values, axis=-1, keepdims=True)
    centred = values - row_mean
    spread = jnp.mean(centred * centred, axis=-1, keepdims=True)
    return centred * lax.rsqrt(spread + EPSILON) * scales


def combine_states(earlier_pair, later_pair):
    return (
        earlier_pair[0] * later_pair[1][..., None, None] + later_pair[0],
        earlier_pair[1] * later_pair[1],
    )


def chain_step(state_now, inputs):
    fresh_one, decay_one = inputs
    return (state_now * decay_one[..., None, None] + fresh_one, state_now)


def plain_shards(
    incoming_residual_stream,
    result_valve,
    channel_feed_matrix,
    memory_feed_matrix,
    memory_query_matrix,
    unsoftened_deltas,
    delta_offset,
    channel_fading_speed,
    extra_log_fading,
    bypass_factor,
    channel_feed_kernel,
    memory_feed_kernel,
    memory_query_kernel,
    cluster_scaling_vector,
    mixer_result_matrix,
    initial_scaling_vector,
    valve_matrix,
    widen_matrix,
    shrink_matrix,
    valve_filter_kernel,
    widen_filter_kernel,
    latter_scaling_vector,
):
    row_count = channel_feed_matrix.shape[0]
    inner_here = channel_feed_matrix.shape[1]
    group_count = memory_feed_matrix.shape[1] // STATE
    group_heads = HEADS // GROUPS
    block_count = row_count // BLOCK
    rim_rows = CONV - 1
    rim_x, rim_b, rim_c = shifted(
        (
            channel_feed_matrix[row_count - rim_rows :],
            memory_feed_matrix[row_count - rim_rows :],
            memory_query_matrix[row_count - rim_rows :],
        ),
        "sp",
        1,
    )
    x_act = jax.nn.silu(causal_conv(channel_feed_matrix, rim_x, channel_feed_kernel)).astype(
        jnp.bfloat16
    )
    b_act = jax.nn.silu(causal_conv(memory_feed_matrix, rim_b, memory_feed_kernel)).astype(
        jnp.bfloat16
    )
    c_act = jax.nn.silu(causal_conv(memory_query_matrix, rim_c, memory_query_kernel)).astype(
        jnp.bfloat16
    )
    channel_delta_amount = jax.nn.softplus(unsoftened_deltas + delta_offset[None, :])
    log_fading_amount = extra_log_fading - channel_fading_speed[None, :] * channel_delta_amount
    x_heads = x_act.astype(jnp.float32).reshape(row_count, group_count, group_heads, HEAD_DIM)
    x_scaled = (
        x_heads * channel_delta_amount.reshape(row_count, group_count, group_heads)[..., None]
    )
    b_full = b_act.astype(jnp.float32).reshape(row_count, group_count, STATE)
    c_full = c_act.astype(jnp.float32).reshape(row_count, group_count, STATE)
    decay_full = log_fading_amount.reshape(row_count, group_count, group_heads)
    x_blk = x_scaled.reshape(block_count, BLOCK, group_count, group_heads, HEAD_DIM)
    b_blk = b_full.reshape(block_count, BLOCK, group_count, STATE)
    c_blk = c_full.reshape(block_count, BLOCK, group_count, STATE)
    b_narrow = b_act.reshape(block_count, BLOCK, group_count, STATE)
    c_narrow = c_act.reshape(block_count, BLOCK, group_count, STATE)
    decay_blk = decay_full.reshape(block_count, BLOCK, group_count, group_heads)
    cum_decay = jnp.cumsum(decay_blk, axis=1)
    causal = jnp.tril(jnp.ones((BLOCK, BLOCK), dtype=bool))
    between = cum_decay[:, :, None] - cum_decay[:, None, :]
    lag = jnp.exp(jnp.where(causal[None, :, :, None, None], between, -jnp.inf))
    affinity = jnp.einsum("blgn,bsgn->blsg", c_narrow, b_narrow, preferred_element_type=jnp.float32)
    mixing = affinity[..., None] * lag
    within = jnp.einsum("blsgh,bsghp->blghp", mixing, x_blk, precision=HIGHEST)
    to_end = jnp.exp(cum_decay[:, -1:] - cum_decay)
    fresh = jnp.einsum("blgn,blghp->bghpn", b_blk, x_blk * to_end[..., None], precision=HIGHEST)
    block_decay = jnp.exp(cum_decay[:, -1])
    initial = jnp.zeros((group_count, group_heads, HEAD_DIM, STATE), jnp.float32)
    local_end, earlier = lax.scan(chain_step, initial, (fresh, block_decay))
    carried = (
        jnp.einsum("blgn,bghpn->blghp", c_blk, earlier, precision=HIGHEST)
        * jnp.exp(cum_decay)[..., None]
    )
    from_start = jnp.cumsum(decay_full, axis=0)
    incoming, _ = entering(
        (local_end, jnp.exp(from_start[-1])),
        "sp",
        combine_states,
        (jnp.zeros_like(local_end), jnp.ones_like(from_start[-1])),
    )
    arriving = (
        jnp.einsum("tgn,ghpn->tghp", c_full, incoming, precision=HIGHEST)
        * jnp.exp(from_start)[..., None]
    )
    y_heads = (within + carried).reshape(row_count, group_count, group_heads, HEAD_DIM) + arriving
    y_heads = y_heads + bypass_factor.reshape(group_count, group_heads)[None, :, :, None] * x_heads
    gated = y_heads.reshape(row_count, group_count, group_heads * HEAD_DIM)
    gated = gated * jax.nn.silu(result_valve.astype(jnp.float32)).reshape(
        row_count, group_count, group_heads * HEAD_DIM
    )
    gated = gated * lax.rsqrt(jnp.mean(gated * gated, axis=-1, keepdims=True) + EPSILON)
    y_norm = (gated.reshape(row_count, inner_here) * cluster_scaling_vector[None, :]).astype(
        jnp.bfloat16
    )
    mixer = lax.psum_scatter(
        jnp.dot(y_norm, mixer_result_matrix, preferred_element_type=jnp.float32).astype(
            jnp.bfloat16
        ),
        "tp",
        scatter_dimension=0,
        tiled=True,
    ).astype(jnp.float32)
    normed_own = layer_norm(
        ALPHA * incoming_residual_stream.astype(jnp.float32) + mixer, initial_scaling_vector
    ).astype(jnp.bfloat16)
    normed_all = lax.all_gather(normed_own, "tp", axis=0, tiled=True)
    gate_sum = jnp.dot(
        normed_all,
        lax.all_gather(valve_matrix, "sp", axis=0, tiled=True),
        preferred_element_type=jnp.float32,
    )
    up_sum = jnp.dot(
        normed_all,
        lax.all_gather(widen_matrix, "sp", axis=0, tiled=True),
        preferred_element_type=jnp.float32,
    )
    gate_proj = gate_sum.astype(jnp.bfloat16)
    up_proj = up_sum.astype(jnp.bfloat16)
    ffn_rows = FCONV - 1
    rim_gate, rim_up = shifted(
        (gate_proj[row_count - ffn_rows :], up_proj[row_count - ffn_rows :]), "sp", 1
    )
    gate_conv = causal_conv(gate_proj, rim_gate, valve_filter_kernel)
    up_conv = causal_conv(up_proj, rim_up, widen_filter_kernel)
    hidden = (jax.nn.silu(gate_conv) * up_conv).astype(jnp.bfloat16)
    channel_part = jnp.dot(
        hidden,
        lax.all_gather(shrink_matrix, "sp", axis=1, tiled=True),
        preferred_element_type=jnp.float32,
    )
    channel = lax.psum_scatter(
        channel_part.astype(jnp.bfloat16), "tp", scatter_dimension=0, tiled=True
    ).astype(jnp.float32)
    return layer_norm(
        ALPHA * normed_own.astype(jnp.float32) + channel, latter_scaling_vector
    ).astype(jnp.bfloat16)


MESH = pl.DeviceIdType.MESH
RIM = 16


def silu(v):
    return v / (1.0 + jnp.exp(-v))


def layer_kernel(
    n_sp,
    n_tp,
    res_ref,
    rv_ref,
    xf_ref,
    bf_ref,
    cf_ref,
    dt_ref,
    doff_ref,
    fade_ref,
    elf_ref,
    byp_ref,
    xk_ref,
    bk_ref,
    ck_ref,
    csv_ref,
    mm_ref,
    g1_ref,
    v_hbm,
    w_hbm,
    s_hbm,
    vk_ref,
    wk_ref,
    g2_ref,
    out_ref,
    v_all,
    w_all,
    s_all,
    rim_x,
    rim_b,
    rim_c,
    ext,
    x_act,
    b_act,
    c_act,
    step_ref,
    ld_ref,
    y_ref,
    efs_ref,
    base_ref,
    state_ref,
    st_send,
    dec_send,
    st_recv,
    dec_recv,
    part,
    recv1,
    recv2,
    normed,
    hidden,
    own_sem,
    ring_send,
    ring_recv,
    rim_send,
    rim_recv,
    st_ssem,
    st_rsem,
    t1_send,
    t1_recv,
    t2_send,
    t2_recv,
    t3_send,
    t3_recv,
    nr_send,
    nr_recv,
):
    f32, bf16 = jnp.float32, jnp.bfloat16
    rows, inner = xf_ref.shape
    heads = dt_ref.shape[1]
    own_rows = rows // n_tp
    width = mm_ref.shape[1]
    ff = v_hbm.shape[1]
    depth = v_hbm.shape[0]
    cols = s_hbm.shape[1]
    blocks = rows // BLOCK
    me = lax.axis_index("sp")
    mt = lax.axis_index("tp")
    half = n_sp // 2

    def owner(pos):
        back = pos // half
        return (1 - back) * 2 * pos + back * (2 * (n_sp - 1 - pos) + 1)

    odd = me % 2
    place = (1 - odd) * (me // 2) + odd * (n_sp - 1 - me // 2)
    after = owner((place + 1) % n_sp)
    ahead = owner((place + n_sp - 1) % n_sp)

    barrier = pltpu.get_barrier_semaphore()
    for d in range(1, n_sp):
        pl.semaphore_signal(barrier, inc=1, device_id=((me + d) % n_sp, mt), device_id_type=MESH)
    for d in range(1, n_tp):
        pl.semaphore_signal(barrier, inc=1, device_id=(me, (mt + d) % n_tp), device_id_type=MESH)
    pl.semaphore_wait(barrier, n_sp + n_tp - 2)

    def slot(piece, who):
        if piece == 2:
            return s_all.at[who]
        whole = v_all if piece == 0 else w_all
        return whole.at[pl.ds(pl.multiple_of(who * depth, depth), depth)]

    sources = (v_hbm, w_hbm, s_hbm)
    hops = {}
    for piece in range(3):
        long_way = half if piece != 1 else n_sp - 1 - half
        hops[piece] = (long_way, n_sp - 1 - long_way)

    def ring_copy(piece, way, step):
        who = owner((place + n_sp - step) % n_sp if way == 0 else (place + step) % n_sp)
        return pltpu.make_async_remote_copy(
            src_ref=sources[piece] if step == 0 else slot(piece, who),
            dst_ref=slot(piece, who),
            send_sem=ring_send.at[way, step, piece],
            recv_sem=ring_recv.at[way, step, piece],
            device_id=(after if way == 0 else ahead, mt),
            device_id_type=MESH,
        )

    def advance(piece, step):
        for way in range(2):
            if 1 <= step <= hops[piece][way]:
                ring_copy(piece, way, step - 1).wait_recv()
            if step < hops[piece][way]:
                ring_copy(piece, way, step).start()

    rim_copies = []
    for i, (a, b) in enumerate(((xf_ref, rim_x), (bf_ref, rim_b), (cf_ref, rim_c))):
        rim_copies.append(
            pltpu.make_async_remote_copy(
                src_ref=a.at[pl.ds(rows - RIM, RIM)],
                dst_ref=b,
                send_sem=rim_send.at[i],
                recv_sem=rim_recv.at[i],
                device_id=((me + 1) % n_sp, mt),
                device_id_type=MESH,
            )
        )
        rim_copies[-1].start()
    own_copies = []
    for piece in range(3):
        advance(piece, 0)
        own_copies.append(
            pltpu.make_async_copy(sources[piece], slot(piece, me), own_sem.at[piece])
        )
        own_copies[-1].start()

    raw = dt_ref[...] + doff_ref[...]
    step_ref[...] = jnp.maximum(raw, 0.0) + jnp.log1p(jnp.exp(-jnp.abs(raw)))
    ld_ref[...] = elf_ref[...] - fade_ref[...] * step_ref[...]

    for c in rim_copies:
        c.wait_recv()
    first = me == 0
    for rim, feed, taps, act in (
        (rim_x, xf_ref, xk_ref, x_act),
        (rim_b, bf_ref, bk_ref, b_act),
        (rim_c, cf_ref, ck_ref, c_act),
    ):
        for lo in range(0, feed.shape[1], 128):
            here = slice(lo, lo + 128)
            edge = rim[:, here].astype(f32)
            ext[0:RIM, :] = jnp.where(first, jnp.zeros_like(edge), edge)
            ext[RIM:, :] = feed[:, here].astype(f32)
            tap = taps[:, here].astype(f32)
            total = jnp.zeros((rows, 128), f32)
            for k in range(CONV):
                start = RIM - (CONV - 1) + k
                total = total + tap[k : k + 1] * ext[start : start + rows, :]
            act[:, here] = silu(total).astype(bf16)

    li = lax.broadcasted_iota(jnp.int32, (BLOCK, BLOCK), 0)
    si = lax.broadcasted_iota(jnp.int32, (BLOCK, BLOCK), 1)
    causal = li >= si
    lower = jnp.where(causal, 1.0, 0.0).astype(f32)
    upper = jnp.where(li <= si, 1.0, 0.0).astype(f32)
    spread = jnp.where(
        lax.broadcasted_iota(jnp.int32, (heads, inner), 1) // HEAD_DIM
        == lax.broadcasted_iota(jnp.int32, (heads, inner), 0),
        1.0,
        0.0,
    ).astype(f32)
    near = lax.broadcasted_iota(jnp.int32, (BLOCK, 2 * HEAD_DIM), 1) < HEAD_DIM

    def widen(a):
        return jnp.dot(a, spread, precision=HIGHEST, preferred_element_type=f32)

    state_ref[...] = jnp.zeros_like(state_ref)
    base_ref[...] = jnp.zeros_like(base_ref)
    skip = widen(byp_ref[...])

    def scan_block(b, carry):
        at = pl.ds(pl.multiple_of(b * BLOCK, BLOCK), BLOCK)
        ld = ld_ref[at, :]
        cum = jnp.dot(lower, ld, precision=HIGHEST, preferred_element_type=f32)
        cum_t = lax.dot_general(
            ld, upper, (((0,), (0,)), ((), ())), precision=HIGHEST, preferred_element_type=f32
        )
        last = cum[BLOCK - 1 : BLOCK, :]
        x = x_act[at, :].astype(f32)
        bb = b_act[at, :]
        cc = c_act[at, :]
        xs = x * widen(step_ref[at, :])
        xs16 = xs.astype(bf16)
        aff = lax.dot_general(
            cc, bb, (((1,), (1,)), ((), ())), preferred_element_type=f32
        )
        y = (
            jnp.dot(cc, state_ref[...].astype(bf16), preferred_element_type=f32)
            * widen(jnp.exp(cum))
            + skip * x
        )
        for pair in range(heads // 2):
            at_pair = slice(pair * 2 * HEAD_DIM, (pair + 1) * 2 * HEAD_DIM)
            both = []
            for h in (2 * pair, 2 * pair + 1):
                gap = cum[:, h : h + 1] - cum_t[h : h + 1, :]
                lag = jnp.exp(jnp.where(causal, gap, -1e30))
                both.append(
                    jnp.dot(
                        (aff * lag).astype(bf16), xs16[:, at_pair], preferred_element_type=f32
                    )
                )
            y_ref[at, at_pair] = y[:, at_pair] + jnp.where(near, both[0], both[1])
        fresh = lax.dot_general(
            bb,
            (xs * widen(jnp.exp(last - cum))).astype(bf16),
            (((0,), (0,)), ((), ())),
            preferred_element_type=f32,
        )
        state_ref[...] = state_ref[...] * widen(jnp.exp(last)) + fresh
        base = base_ref[0:1, :]
        efs_ref[at, :] = jnp.exp(base + cum)
        base_ref[0:1, :] = base + last
        return carry

    lax.fori_loop(0, blocks, scan_block, 0)
    st_send[...] = state_ref[...].astype(bf16)
    dec_send[...] = jnp.broadcast_to(widen(jnp.exp(base_ref[0:1, :])), dec_send.shape)

    def state_copies(d):
        to = ((me + d) % n_sp, mt)
        return [
            pltpu.make_async_remote_copy(
                src_ref=a,
                dst_ref=b.at[d],
                send_sem=st_ssem.at[d, i],
                recv_sem=st_rsem.at[d, i],
                device_id=to,
                device_id_type=MESH,
            )
            for i, (a, b) in enumerate(((st_send, st_recv), (dec_send, dec_recv)))
        ]

    state_ref[...] = jnp.zeros_like(state_ref)
    for d in range(1, n_sp):

        @pl.when(me + d < n_sp)
        def _(d=d):
            for c in state_copies(d):
                c.start()

    advance(0, 1)
    advance(1, 1)
    for d in range(n_sp - 1, 0, -1):

        @pl.when(me >= d)
        def _(d=d):
            for c in state_copies(d):
                c.wait_recv()
            state_ref[...] = state_ref[...] * dec_recv[d, 0:1, :] + st_recv[d].astype(f32)

    def project_block(b, carry):
        at = pl.ds(pl.multiple_of(b * BLOCK, BLOCK), BLOCK)
        y = y_ref[at, :] + jnp.dot(
            c_act[at, :], state_ref[...].astype(bf16), preferred_element_type=f32
        ) * widen(efs_ref[at, :])
        gated = y * silu(rv_ref[at, :].astype(f32))
        gated = gated * lax.rsqrt(jnp.mean(gated * gated, axis=-1, keepdims=True) + EPSILON)
        y_norm = (gated * csv_ref[...]).astype(bf16)
        part[at, :] = jnp.dot(y_norm, mm_ref[...], preferred_element_type=f32).astype(bf16)
        return carry

    lax.fori_loop(0, blocks, project_block, 0)

    def rows_of(t):
        return pl.ds(pl.multiple_of(t * own_rows, own_rows), own_rows)

    def tp_copy(d, src, dst, send, recv):
        return pltpu.make_async_remote_copy(
            src_ref=src,
            dst_ref=dst,
            send_sem=send,
            recv_sem=recv,
            device_id=(me, (mt + d) % n_tp),
            device_id_type=MESH,
        )

    first_sum = [
        tp_copy(d, part.at[rows_of((mt + d) % n_tp)], recv1.at[d], t1_send.at[d], t1_recv.at[d])
        for d in range(1, n_tp)
    ]
    for c in first_sum:
        c.start()
    advance(0, 2)
    for c in first_sum:
        c.wait_recv()
    mixer = part[rows_of(mt), :].astype(f32)
    for d in range(1, n_tp):
        mixer = mixer + recv1[d].astype(f32)
    mine = pl.ds(pl.multiple_of(RIM + mt * own_rows, RIM), own_rows)
    normed[mine, :] = layer_norm(
        ALPHA * res_ref[...].astype(f32) + mixer, g1_ref[...]
    ).astype(bf16)
    for c in first_sum:
        c.wait_send()
    spread_rows = [
        tp_copy(d, normed.at[mine], normed.at[mine], t2_send.at[d], t2_recv.at[d])
        for d in range(1, n_tp)
    ]
    for c in spread_rows:
        c.start()
    advance(1, 2)
    advance(0, 3)
    for c in spread_rows:
        c.wait()
    rim_norm = pltpu.make_async_remote_copy(
        src_ref=normed.at[pl.ds(rows, RIM)],
        dst_ref=normed.at[pl.ds(0, RIM)],
        send_sem=nr_send,
        recv_sem=nr_recv,
        device_id=((me + 1) % n_sp, mt),
        device_id_type=MESH,
    )

    @pl.when(me + 1 < n_sp)
    def _():
        rim_norm.start()

    @pl.when(me == 0)
    def _():
        normed[0:RIM, :] = jnp.zeros((RIM, width), bf16)

    advance(1, 3)
    advance(2, 1)
    for s in range(4, half + 1):
        advance(0, s)
        advance(1, s)

    @pl.when(me > 0)
    def _():
        rim_norm.wait_recv()

    for c in own_copies:
        c.wait()

    def ffn_cols(at):
        feeds = normed[...]
        convs = []
        for weights, taps in ((v_all, vk_ref), (w_all, wk_ref)):
            proj = jnp.dot(feeds, weights[:, at], preferred_element_type=f32)
            proj = proj.astype(bf16).astype(f32)
            tap = taps[:, at].astype(f32)
            total = jnp.zeros((rows, proj.shape[1]), f32)
            for k in range(FCONV):
                start = RIM - (FCONV - 1) + k
                total = total + tap[k : k + 1] * proj[start : start + rows, :]
            convs.append(total)
        hidden[:, at] = (silu(convs[0]) * convs[1]).astype(bf16)

    chunk = 256
    full = ff // chunk

    def ffn_chunk(i, carry):
        ffn_cols(pl.ds(pl.multiple_of(i * chunk, chunk), chunk))
        return carry

    lax.fori_loop(0, full // 2, ffn_chunk, 0)
    advance(2, 2)
    lax.fori_loop(full // 2, full, ffn_chunk, 0)
    if ff % chunk:
        ffn_cols(pl.ds(full * chunk, ff % chunk))

    def down(who):
        at = pl.ds(pl.multiple_of(who * cols, cols), cols)
        part[:, at] = jnp.dot(
            hidden[...], s_all[who], preferred_element_type=f32
        ).astype(bf16)

    def down_copies(who):
        at = pl.ds(pl.multiple_of(who * cols, cols), cols)
        return [
            tp_copy(
                d,
                part.at[rows_of((mt + d) % n_tp), at],
                recv2.at[d, :, at],
                t3_send.at[d, who],
                t3_recv.at[d, who],
            )
            for d in range(1, n_tp)
        ]

    down(me)
    for c in down_copies(me):
        c.start()
    for k in range(1, half + 1):
        if k >= 3:
            advance(2, k)
        count = 2 if k < half else 1

        def both_ways(q, carry, k=k):
            who = owner((place + n_sp - k + 2 * k * q) % n_sp)
            down(who)
            for c in down_copies(who):
                c.start()
            return carry

        lax.fori_loop(0, count, both_ways, 0)

    def settle(who, carry):
        for c in down_copies(who):
            c.wait()
        return carry

    lax.fori_loop(0, n_sp, settle, 0)
    channel = part[rows_of(mt), :].astype(f32)
    for d in range(1, n_tp):
        channel = channel + recv2[d].astype(f32)
    out_ref[...] = layer_norm(
        ALPHA * normed[mine, :].astype(f32) + channel, g2_ref[...]
    ).astype(bf16)

    for piece in range(3):
        for way in range(2):
            for s in range(hops[piece][way]):
                ring_copy(piece, way, s).wait_send()
    for c in rim_copies:
        c.wait_send()

    @pl.when(me + 1 < n_sp)
    def _():
        rim_norm.wait_send()

    for d in range(1, n_sp):

        @pl.when(me + d < n_sp)
        def _(d=d):
            for c in state_copies(d):
                c.wait_send()


def fused_shards(n_sp, n_tp, *args):
    (
        res, rv, xf, bf, cf, dt, doff, fade, elf, byp, xk, bk, ck, csv, mm, g1, v, w, s, vk, wk, g2
    ) = args
    f32, bf16 = jnp.float32, jnp.bfloat16
    rows, inner = xf.shape
    heads = dt.shape[1]
    width = mm.shape[1]
    ff = v.shape[1]
    row = lambda a: a.reshape(1, -1)
    half = n_sp // 2
    vmem = pl.BlockSpec(memory_space=pltpu.VMEM)
    hbm = pl.BlockSpec(memory_space=pl.ANY)
    dma = pltpu.SemaphoreType.DMA
    return pl.pallas_call(
        functools.partial(layer_kernel, n_sp, n_tp),
        out_shape=jax.ShapeDtypeStruct(res.shape, bf16),
        in_specs=[vmem] * 16 + [hbm] * 3 + [vmem] * 3,
        out_specs=vmem,
        scratch_shapes=[
            pltpu.VMEM((n_sp * v.shape[0], ff), bf16),
            pltpu.VMEM((n_sp * v.shape[0], ff), bf16),
            pltpu.VMEM((n_sp,) + s.shape, bf16),
            pltpu.VMEM((RIM, inner), bf16),
            pltpu.VMEM((RIM, STATE), bf16),
            pltpu.VMEM((RIM, STATE), bf16),
            pltpu.VMEM((rows + RIM, 128), f32),
            pltpu.VMEM((rows, inner), bf16),
            pltpu.VMEM((rows, STATE), bf16),
            pltpu.VMEM((rows, STATE), bf16),
            pltpu.VMEM((rows, heads), f32),
            pltpu.VMEM((rows, heads), f32),
            pltpu.VMEM((rows, inner), f32),
            pltpu.VMEM((rows, heads), f32),
            pltpu.VMEM((8, heads), f32),
            pltpu.VMEM((STATE, inner), f32),
            pltpu.VMEM((STATE, inner), bf16),
            pltpu.VMEM((8, inner), f32),
            pltpu.VMEM((n_sp, STATE, inner), bf16),
            pltpu.VMEM((n_sp, 8, inner), f32),
            pltpu.VMEM((rows, width), bf16),
            pltpu.VMEM((n_tp, rows // n_tp, width), bf16),
            pltpu.VMEM((n_tp, rows // n_tp, width), bf16),
            pltpu.VMEM((rows + RIM, width), bf16),
            pltpu.VMEM((rows, ff), bf16),
            dma((3,)),
            dma((2, half, 3)),
            dma((2, half, 3)),
            dma((3,)),
            dma((3,)),
            dma((n_sp, 2)),
            dma((n_sp, 2)),
            dma((n_tp,)),
            dma((n_tp,)),
            dma((n_tp,)),
            dma((n_tp,)),
            dma((n_tp, n_sp)),
            dma((n_tp, n_sp)),
            dma,
            dma,
        ],
        compiler_params=pltpu.CompilerParams(
            collective_id=0, has_side_effects=True, vmem_limit_bytes=60 * 1024 * 1024
        ),
    )(
        res, rv, xf, bf, cf, dt, row(doff), row(fade), elf, row(byp), xk, bk, ck, row(csv), mm,
        row(g1), v, w, s, vk, wk, row(g2),
    )


def shards_for(n_sp, n_tp):
    def shards(*args):
        rows = args[2].shape[0]
        fits = (
            args[3].shape[1] == STATE
            and args[18].shape[1] % 128 == 0
            and args[16].shape[0] % 16 == 0
            and args[16].shape[1] % 128 == 0
            and n_sp % 2 == 0
            and rows % (BLOCK * n_tp) == 0
        )
        if fits:
            return fused_shards(n_sp, n_tp, *args)
        return plain_shards(*args)

    return shards


def solution(mesh):
    in_specs = (
        P(("sp", "tp"), None),
        P("sp", "tp"),
        P("sp", "tp"),
        P("sp", "tp"),
        P("sp", "tp"),
        P("sp", "tp"),
        P("tp"),
        P("tp"),
        P("sp", "tp"),
        P("tp"),
        P(None, "tp"),
        P(None, "tp"),
        P(None, "tp"),
        P("tp"),
        P("tp", None),
        P(),
        P("sp", "tp"),
        P("sp", "tp"),
        P("tp", "sp"),
        P(None, "tp"),
        P(None, "tp"),
        P(),
    )
    out_specs = P(("sp", "tp"), None)
    shards = shards_for(mesh.shape["sp"], mesh.shape["tp"])
    return jax.shard_map(shards, mesh=mesh, in_specs=in_specs, out_specs=out_specs, check_vma=False)
```

```python
import functools
import jax
import jax.numpy as jnp
from jax import lax
from jax.experimental import pallas as pl
from jax.experimental.pallas import tpu as pltpu
from jax.sharding import PartitionSpec as P

HEADS = 32
HEAD_DIM = 64
GROUPS = 4
STATE = 128
CONV = 4
FCONV = 3
BLOCK = 128


EPSILON = 1e-05
ALPHA = 2.0**0.25
HIGHEST = lax.Precision.HIGHEST


def shifted(shard, axis, by):
    count = lax.axis_size(axis)
    pairs = [(i, i + by) for i in range(count) if 0 <= i + by < count]
    return lax.ppermute(shard, axis, pairs)


def entering(shard, axis, join, neutral):
    place = lax.axis_index(axis)
    gathered = jax.tree.map(
        lambda a, kind: lax.all_gather(a.astype(kind), axis), shard, (jnp.bfloat16, jnp.bfloat16)
    )
    state = jax.tree.map(lambda a, e: jnp.zeros_like(a) + jnp.asarray(e, a.dtype), shard, neutral)

    def one(lap, state):
        return join(
            state,
            jax.tree.map(
                lambda a, own: lax.dynamic_index_in_dim(a, lap, 0, False).astype(own.dtype),
                gathered,
                shard,
            ),
        )

    return lax.fori_loop(0, place, one, state)


def causal_conv(signal, before, tap_weights):
    tap_count = tap_weights.shape[0]
    row_count = signal.shape[0]
    padded = jnp.concatenate([before, signal], axis=0).astype(jnp.float32)
    running = jnp.zeros(signal.shape, jnp.float32)
    for tap_index in range(tap_count):
        running = (
            running
            + tap_weights[tap_index].astype(jnp.float32) * padded[tap_index : tap_index + row_count]
        )
    return running


def layer_norm(values, scales):
    row_mean = jnp.mean(values, axis=-1, keepdims=True)
    centred = values - row_mean
    spread = jnp.mean(centred * centred, axis=-1, keepdims=True)
    return centred * lax.rsqrt(spread + EPSILON) * scales


def combine_states(earlier_pair, later_pair):
    return (
        earlier_pair[0] * later_pair[1][..., None, None] + later_pair[0],
        earlier_pair[1] * later_pair[1],
    )


def chain_step(state_now, inputs):
    fresh_one, decay_one = inputs
    return (state_now * decay_one[..., None, None] + fresh_one, state_now)


def plain_shards(
    incoming_residual_stream,
    result_valve,
    channel_feed_matrix,
    memory_feed_matrix,
    memory_query_matrix,
    unsoftened_deltas,
    delta_offset,
    channel_fading_speed,
    extra_log_fading,
    bypass_factor,
    channel_feed_kernel,
    memory_feed_kernel,
    memory_query_kernel,
    cluster_scaling_vector,
    mixer_result_matrix,
    initial_scaling_vector,
    valve_matrix,
    widen_matrix,
    shrink_matrix,
    valve_filter_kernel,
    widen_filter_kernel,
    latter_scaling_vector,
):
    row_count = channel_feed_matrix.shape[0]
    inner_here = channel_feed_matrix.shape[1]
    group_count = memory_feed_matrix.shape[1] // STATE
    group_heads = HEADS // GROUPS
    block_count = row_count // BLOCK
    rim_rows = CONV - 1
    rim_x, rim_b, rim_c = shifted(
        (
            channel_feed_matrix[row_count - rim_rows :],
            memory_feed_matrix[row_count - rim_rows :],
            memory_query_matrix[row_count - rim_rows :],
        ),
        "sp",
        1,
    )
    x_act = jax.nn.silu(causal_conv(channel_feed_matrix, rim_x, channel_feed_kernel)).astype(
        jnp.bfloat16
    )
    b_act = jax.nn.silu(causal_conv(memory_feed_matrix, rim_b, memory_feed_kernel)).astype(
        jnp.bfloat16
    )
    c_act = jax.nn.silu(causal_conv(memory_query_matrix, rim_c, memory_query_kernel)).astype(
        jnp.bfloat16
    )
    channel_delta_amount = jax.nn.softplus(unsoftened_deltas + delta_offset[None, :])
    log_fading_amount = extra_log_fading - channel_fading_speed[None, :] * channel_delta_amount
    x_heads = x_act.astype(jnp.float32).reshape(row_count, group_count, group_heads, HEAD_DIM)
    x_scaled = (
        x_heads * channel_delta_amount.reshape(row_count, group_count, group_heads)[..., None]
    )
    b_full = b_act.astype(jnp.float32).reshape(row_count, group_count, STATE)
    c_full = c_act.astype(jnp.float32).reshape(row_count, group_count, STATE)
    decay_full = log_fading_amount.reshape(row_count, group_count, group_heads)
    x_blk = x_scaled.reshape(block_count, BLOCK, group_count, group_heads, HEAD_DIM)
    b_blk = b_full.reshape(block_count, BLOCK, group_count, STATE)
    c_blk = c_full.reshape(block_count, BLOCK, group_count, STATE)
    b_narrow = b_act.reshape(block_count, BLOCK, group_count, STATE)
    c_narrow = c_act.reshape(block_count, BLOCK, group_count, STATE)
    decay_blk = decay_full.reshape(block_count, BLOCK, group_count, group_heads)
    cum_decay = jnp.cumsum(decay_blk, axis=1)
    causal = jnp.tril(jnp.ones((BLOCK, BLOCK), dtype=bool))
    between = cum_decay[:, :, None] - cum_decay[:, None, :]
    lag = jnp.exp(jnp.where(causal[None, :, :, None, None], between, -jnp.inf))
    affinity = jnp.einsum("blgn,bsgn->blsg", c_narrow, b_narrow, preferred_element_type=jnp.float32)
    mixing = affinity[..., None] * lag
    within = jnp.einsum("blsgh,bsghp->blghp", mixing, x_blk, precision=HIGHEST)
    to_end = jnp.exp(cum_decay[:, -1:] - cum_decay)
    fresh = jnp.einsum("blgn,blghp->bghpn", b_blk, x_blk * to_end[..., None], precision=HIGHEST)
    block_decay = jnp.exp(cum_decay[:, -1])
    initial = jnp.zeros((group_count, group_heads, HEAD_DIM, STATE), jnp.float32)
    local_end, earlier = lax.scan(chain_step, initial, (fresh, block_decay))
    carried = (
        jnp.einsum("blgn,bghpn->blghp", c_blk, earlier, precision=HIGHEST)
        * jnp.exp(cum_decay)[..., None]
    )
    from_start = jnp.cumsum(decay_full, axis=0)
    incoming, _ = entering(
        (local_end, jnp.exp(from_start[-1])),
        "sp",
        combine_states,
        (jnp.zeros_like(local_end), jnp.ones_like(from_start[-1])),
    )
    arriving = (
        jnp.einsum("tgn,ghpn->tghp", c_full, incoming, precision=HIGHEST)
        * jnp.exp(from_start)[..., None]
    )
    y_heads = (within + carried).reshape(row_count, group_count, group_heads, HEAD_DIM) + arriving
    y_heads = y_heads + bypass_factor.reshape(group_count, group_heads)[None, :, :, None] * x_heads
    gated = y_heads.reshape(row_count, group_count, group_heads * HEAD_DIM)
    gated = gated * jax.nn.silu(result_valve.astype(jnp.float32)).reshape(
        row_count, group_count, group_heads * HEAD_DIM
    )
    gated = gated * lax.rsqrt(jnp.mean(gated * gated, axis=-1, keepdims=True) + EPSILON)
    y_norm = (gated.reshape(row_count, inner_here) * cluster_scaling_vector[None, :]).astype(
        jnp.bfloat16
    )
    mixer = lax.psum_scatter(
        jnp.dot(y_norm, mixer_result_matrix, preferred_element_type=jnp.float32).astype(
            jnp.bfloat16
        ),
        "tp",
        scatter_dimension=0,
        tiled=True,
    ).astype(jnp.float32)
    normed_own = layer_norm(
        ALPHA * incoming_residual_stream.astype(jnp.float32) + mixer, initial_scaling_vector
    ).astype(jnp.bfloat16)
    normed_all = lax.all_gather(normed_own, "tp", axis=0, tiled=True)
    gate_sum = jnp.dot(
        normed_all,
        lax.all_gather(valve_matrix, "sp", axis=0, tiled=True),
        preferred_element_type=jnp.float32,
    )
    up_sum = jnp.dot(
        normed_all,
        lax.all_gather(widen_matrix, "sp", axis=0, tiled=True),
        preferred_element_type=jnp.float32,
    )
    gate_proj = gate_sum.astype(jnp.bfloat16)
    up_proj = up_sum.astype(jnp.bfloat16)
    ffn_rows = FCONV - 1
    rim_gate, rim_up = shifted(
        (gate_proj[row_count - ffn_rows :], up_proj[row_count - ffn_rows :]), "sp", 1
    )
    gate_conv = causal_conv(gate_proj, rim_gate, valve_filter_kernel)
    up_conv = causal_conv(up_proj, rim_up, widen_filter_kernel)
    hidden = (jax.nn.silu(gate_conv) * up_conv).astype(jnp.bfloat16)
    channel_part = jnp.dot(
        hidden,
        lax.all_gather(shrink_matrix, "sp", axis=1, tiled=True),
        preferred_element_type=jnp.float32,
    )
    channel = lax.psum_scatter(
        channel_part.astype(jnp.bfloat16), "tp", scatter_dimension=0, tiled=True
    ).astype(jnp.float32)
    return layer_norm(
        ALPHA * normed_own.astype(jnp.float32) + channel, latter_scaling_vector
    ).astype(jnp.bfloat16)


MESH = pl.DeviceIdType.MESH
RIM = 16


def silu(v):
    return v / (1.0 + jnp.exp(-v))


def layer_kernel(
    n_sp,
    n_tp,
    res_ref,
    rv_ref,
    xf_ref,
    bf_ref,
    cf_ref,
    dt_ref,
    doff_ref,
    fade_ref,
    elf_ref,
    byp_ref,
    xk_ref,
    bk_ref,
    ck_ref,
    csv_ref,
    mm_ref,
    g1_ref,
    v_hbm,
    w_hbm,
    s_hbm,
    vk_ref,
    wk_ref,
    g2_ref,
    out_ref,
    v_all,
    w_all,
    s_all,
    rim_x,
    rim_b,
    rim_c,
    ext,
    x_act,
    b_act,
    c_act,
    step_ref,
    ld_ref,
    y_ref,
    efs_ref,
    base_ref,
    state_ref,
    st_send,
    dec_send,
    pair_send,
    pair_dec,
    st_recv,
    dec_recv,
    part,
    recv1,
    recv2,
    normed,
    hidden,
    own_sem,
    ring_send,
    ring_recv,
    rim_send,
    rim_recv,
    st_ssem,
    st_rsem,
    t1_send,
    t1_recv,
    t2_send,
    t2_recv,
    t3_send,
    t3_recv,
    nr_send,
    nr_recv,
):
    f32, bf16 = jnp.float32, jnp.bfloat16
    rows, inner = xf_ref.shape
    heads = dt_ref.shape[1]
    own_rows = rows // n_tp
    width = mm_ref.shape[1]
    ff = v_hbm.shape[1]
    depth = v_hbm.shape[0]
    cols = s_hbm.shape[1]
    blocks = rows // BLOCK
    me = lax.axis_index("sp")
    mt = lax.axis_index("tp")
    half = n_sp // 2

    def owner(pos):
        back = pos // half
        return (1 - back) * 2 * pos + back * (2 * (n_sp - 1 - pos) + 1)

    odd = me % 2
    place = (1 - odd) * (me // 2) + odd * (n_sp - 1 - me // 2)
    after = owner((place + 1) % n_sp)
    ahead = owner((place + n_sp - 1) % n_sp)

    barrier = pltpu.get_barrier_semaphore()
    for d in range(1, n_sp):
        pl.semaphore_signal(barrier, inc=1, device_id=((me + d) % n_sp, mt), device_id_type=MESH)
    for d in range(1, n_tp):
        pl.semaphore_signal(barrier, inc=1, device_id=(me, (mt + d) % n_tp), device_id_type=MESH)
    pl.semaphore_wait(barrier, n_sp + n_tp - 2)

    def slot(piece, who):
        if piece == 2:
            return s_all.at[who]
        whole = v_all if piece == 0 else w_all
        return whole.at[pl.ds(pl.multiple_of(who * depth, depth), depth)]

    sources = (v_hbm, w_hbm, s_hbm)
    hops = {}
    for piece in range(3):
        long_way = half if piece != 1 else n_sp - 1 - half
        hops[piece] = (long_way, n_sp - 1 - long_way) if piece < 2 else (half, half)

    def ring_copy(piece, way, step):
        who = owner((place + n_sp - step) % n_sp if way == 0 else (place + step) % n_sp)
        src = sources[piece] if step == 0 else slot(piece, who)
        dst = slot(piece, who)
        if piece == 2 and step == half - 1:
            part_rows = src.shape[0] // 2
            here = pl.ds(way * part_rows, part_rows)
            src, dst = src.at[here], dst.at[here]
        return pltpu.make_async_remote_copy(
            src_ref=src,
            dst_ref=dst,
            send_sem=ring_send.at[way, step, piece],
            recv_sem=ring_recv.at[way, step, piece],
            device_id=(after if way == 0 else ahead, mt),
            device_id_type=MESH,
        )

    def advance(piece, step):
        for way in range(2):
            if 1 <= step <= hops[piece][way]:
                ring_copy(piece, way, step - 1).wait_recv()
            if step < hops[piece][way]:
                ring_copy(piece, way, step).start()

    rim_copies = []
    for i, (a, b) in enumerate(((xf_ref, rim_x), (bf_ref, rim_b), (cf_ref, rim_c))):
        rim_copies.append(
            pltpu.make_async_remote_copy(
                src_ref=a.at[pl.ds(rows - RIM, RIM)],
                dst_ref=b,
                send_sem=rim_send.at[i],
                recv_sem=rim_recv.at[i],
                device_id=((me + 1) % n_sp, mt),
                device_id_type=MESH,
            )
        )
        rim_copies[-1].start()
    own_copies = []
    for piece in range(3):
        if piece < 2:
            advance(piece, 0)
        own_copies.append(
            pltpu.make_async_copy(sources[piece], slot(piece, me), own_sem.at[piece])
        )
        own_copies[-1].start()

    raw = dt_ref[...] + doff_ref[...]
    step_ref[...] = jnp.maximum(raw, 0.0) + jnp.log1p(jnp.exp(-jnp.abs(raw)))
    ld_ref[...] = elf_ref[...] - fade_ref[...] * step_ref[...]

    for c in rim_copies:
        c.wait_recv()
    first = me == 0
    for rim, feed, taps, act in (
        (rim_x, xf_ref, xk_ref, x_act),
        (rim_b, bf_ref, bk_ref, b_act),
        (rim_c, cf_ref, ck_ref, c_act),
    ):
        for lo in range(0, feed.shape[1], 128):
            here = slice(lo, lo + 128)
            edge = rim[:, here].astype(f32)
            ext[0:RIM, :] = jnp.where(first, jnp.zeros_like(edge), edge)
            ext[RIM:, :] = feed[:, here].astype(f32)
            tap = taps[:, here].astype(f32)
            total = jnp.zeros((rows, 128), f32)
            for k in range(CONV):
                start = RIM - (CONV - 1) + k
                total = total + tap[k : k + 1] * ext[start : start + rows, :]
            act[:, here] = silu(total).astype(bf16)

    li = lax.broadcasted_iota(jnp.int32, (BLOCK, BLOCK), 0)
    si = lax.broadcasted_iota(jnp.int32, (BLOCK, BLOCK), 1)
    causal = li >= si
    lower = jnp.where(causal, 1.0, 0.0).astype(f32)
    upper = jnp.where(li <= si, 1.0, 0.0).astype(f32)
    spread = jnp.where(
        lax.broadcasted_iota(jnp.int32, (heads, inner), 1) // HEAD_DIM
        == lax.broadcasted_iota(jnp.int32, (heads, inner), 0),
        1.0,
        0.0,
    ).astype(f32)
    near = lax.broadcasted_iota(jnp.int32, (BLOCK, 2 * HEAD_DIM), 1) < HEAD_DIM

    def widen(a):
        return jnp.dot(a, spread, precision=HIGHEST, preferred_element_type=f32)

    state_ref[...] = jnp.zeros_like(state_ref)
    base_ref[...] = jnp.zeros_like(base_ref)
    skip = widen(byp_ref[...])

    def scan_block(b, carry):
        at = pl.ds(pl.multiple_of(b * BLOCK, BLOCK), BLOCK)
        ld = ld_ref[at, :]
        cum = jnp.dot(lower, ld, precision=HIGHEST, preferred_element_type=f32)
        cum_t = lax.dot_general(
            ld, upper, (((0,), (0,)), ((), ())), precision=HIGHEST, preferred_element_type=f32
        )
        last = cum[BLOCK - 1 : BLOCK, :]
        x = x_act[at, :].astype(f32)
        bb = b_act[at, :]
        cc = c_act[at, :]
        xs = x * widen(step_ref[at, :])
        xs16 = xs.astype(bf16)
        aff = lax.dot_general(
            cc, bb, (((1,), (1,)), ((), ())), preferred_element_type=f32
        )
        y = (
            jnp.dot(cc, state_ref[...].astype(bf16), preferred_element_type=f32)
            * widen(jnp.exp(cum))
            + skip * x
        )
        for pair in range(heads // 2):
            at_pair = slice(pair * 2 * HEAD_DIM, (pair + 1) * 2 * HEAD_DIM)
            both = []
            for h in (2 * pair, 2 * pair + 1):
                gap = cum[:, h : h + 1] - cum_t[h : h + 1, :]
                lag = jnp.exp(jnp.where(causal, gap, -1e30))
                both.append(
                    jnp.dot(
                        (aff * lag).astype(bf16), xs16[:, at_pair], preferred_element_type=f32
                    )
                )
            y_ref[at, at_pair] = y[:, at_pair] + jnp.where(near, both[0], both[1])
        fresh = lax.dot_general(
            bb,
            (xs * widen(jnp.exp(last - cum))).astype(bf16),
            (((0,), (0,)), ((), ())),
            preferred_element_type=f32,
        )
        state_ref[...] = state_ref[...] * widen(jnp.exp(last)) + fresh
        base = base_ref[0:1, :]
        efs_ref[at, :] = jnp.exp(base + cum)
        base_ref[0:1, :] = base + last
        return carry

    lax.fori_loop(0, blocks, scan_block, 0)
    st_send[...] = state_ref[...].astype(bf16)
    dec_send[...] = jnp.broadcast_to(base_ref[0:1, :], dec_send.shape)
    partner = me + 1 - 2 * odd

    def state_copies(d):
        pair = d > 0
        return [
            pltpu.make_async_remote_copy(
                src_ref=a,
                dst_ref=b.at[d],
                send_sem=st_ssem.at[d, i],
                recv_sem=st_rsem.at[d, i],
                device_id=((me + 2 * d) % n_sp if pair else partner, mt),
                device_id_type=MESH,
            )
            for i, (a, b) in enumerate(
                ((pair_send if pair else st_send, st_recv), (pair_dec if pair else dec_send, dec_recv))
            )
        ]

    for c in state_copies(0):
        c.start()
    advance(0, 1)
    for c in state_copies(0):
        c.wait_recv()
    own_dec = widen(jnp.exp(dec_send[0:1, :]))
    beside_dec = widen(jnp.exp(dec_recv[0, 0:1, :]))
    beside = st_recv[0].astype(f32)
    later = odd == 1
    pair_send[...] = jnp.where(
        later, state_ref[...] + beside * own_dec, state_ref[...] * beside_dec + beside
    ).astype(bf16)
    pair_dec[...] = dec_send[...] + dec_recv[0]
    state_ref[...] = jnp.zeros_like(state_ref)
    for d in range(1, half):

        @pl.when(me + 2 * d < n_sp)
        def _(d=d):
            for c in state_copies(d):
                c.start()

    advance(1, 1)
    advance(2, 0)
    for d in range(half - 1, 0, -1):

        @pl.when(me >= 2 * d)
        def _(d=d):
            for c in state_copies(d):
                c.wait_recv()
            state_ref[...] = state_ref[...] * widen(
                jnp.exp(dec_recv[d, 0:1, :])
            ) + st_recv[d].astype(f32)

    @pl.when(odd == 1)
    def _():
        state_ref[...] = state_ref[...] * widen(jnp.exp(dec_recv[0, 0:1, :])) + st_recv[
            0
        ].astype(f32)

    def project_block(b, carry):
        at = pl.ds(pl.multiple_of(b * BLOCK, BLOCK), BLOCK)
        y = y_ref[at, :] + jnp.dot(
            c_act[at, :], state_ref[...].astype(bf16), preferred_element_type=f32
        ) * widen(efs_ref[at, :])
        gated = y * silu(rv_ref[at, :].astype(f32))
        gated = gated * lax.rsqrt(jnp.mean(gated * gated, axis=-1, keepdims=True) + EPSILON)
        y_norm = (gated * csv_ref[...]).astype(bf16)
        part[at, :] = jnp.dot(y_norm, mm_ref[...], preferred_element_type=f32).astype(bf16)
        return carry

    lax.fori_loop(0, blocks, project_block, 0)

    def rows_of(t):
        return pl.ds(pl.multiple_of(t * own_rows, own_rows), own_rows)

    def tp_copy(d, src, dst, send, recv):
        return pltpu.make_async_remote_copy(
            src_ref=src,
            dst_ref=dst,
            send_sem=send,
            recv_sem=recv,
            device_id=(me, (mt + d) % n_tp),
            device_id_type=MESH,
        )

    first_sum = [
        tp_copy(d, part.at[rows_of((mt + d) % n_tp)], recv1.at[d], t1_send.at[d], t1_recv.at[d])
        for d in range(1, n_tp)
    ]
    for c in first_sum:
        c.start()
    advance(0, 2)
    for c in first_sum:
        c.wait_recv()
    mixer = part[rows_of(mt), :].astype(f32)
    for d in range(1, n_tp):
        mixer = mixer + recv1[d].astype(f32)
    mine = pl.ds(pl.multiple_of(RIM + mt * own_rows, RIM), own_rows)
    normed[mine, :] = layer_norm(
        ALPHA * res_ref[...].astype(f32) + mixer, g1_ref[...]
    ).astype(bf16)
    for c in first_sum:
        c.wait_send()
    spread_rows = [
        tp_copy(d, normed.at[mine], normed.at[mine], t2_send.at[d], t2_recv.at[d])
        for d in range(1, n_tp)
    ]
    for c in spread_rows:
        c.start()
    advance(1, 2)
    advance(0, 3)
    for c in spread_rows:
        c.wait()
    rim_norm = pltpu.make_async_remote_copy(
        src_ref=normed.at[pl.ds(rows, RIM)],
        dst_ref=normed.at[pl.ds(0, RIM)],
        send_sem=nr_send,
        recv_sem=nr_recv,
        device_id=((me + 1) % n_sp, mt),
        device_id_type=MESH,
    )

    @pl.when(me + 1 < n_sp)
    def _():
        rim_norm.start()

    @pl.when(me == 0)
    def _():
        normed[0:RIM, :] = jnp.zeros((RIM, width), bf16)

    advance(1, 3)
    advance(2, 1)
    for s in range(4, half + 1):
        advance(0, s)
        advance(1, s)

    @pl.when(me > 0)
    def _():
        rim_norm.wait_recv()

    for c in own_copies:
        c.wait()

    def ffn_cols(at):
        feeds = normed[...]
        convs = []
        for weights, taps in ((v_all, vk_ref), (w_all, wk_ref)):
            proj = jnp.dot(feeds, weights[:, at], preferred_element_type=f32)
            proj = proj.astype(bf16).astype(f32)
            tap = taps[:, at].astype(f32)
            total = jnp.zeros((rows, proj.shape[1]), f32)
            for k in range(FCONV):
                start = RIM - (FCONV - 1) + k
                total = total + tap[k : k + 1] * proj[start : start + rows, :]
            convs.append(total)
        hidden[:, at] = (silu(convs[0]) * convs[1]).astype(bf16)

    chunk = 256
    full = ff // chunk

    def ffn_chunk(i, carry):
        ffn_cols(pl.ds(pl.multiple_of(i * chunk, chunk), chunk))
        return carry

    lax.fori_loop(0, full // 2, ffn_chunk, 0)
    advance(2, 2)
    lax.fori_loop(full // 2, full, ffn_chunk, 0)
    if ff % chunk:
        ffn_cols(pl.ds(full * chunk, ff % chunk))

    def down(who):
        at = pl.ds(pl.multiple_of(who * cols, cols), cols)
        part[:, at] = jnp.dot(
            hidden[...], s_all[who], preferred_element_type=f32
        ).astype(bf16)

    def down_copies(who):
        at = pl.ds(pl.multiple_of(who * cols, cols), cols)
        return [
            tp_copy(
                d,
                part.at[rows_of((mt + d) % n_tp), at],
                recv2.at[d, :, at],
                t3_send.at[d, who],
                t3_recv.at[d, who],
            )
            for d in range(1, n_tp)
        ]

    down(me)
    for c in down_copies(me):
        c.start()
    for k in range(1, half + 1):
        if k >= 3:
            advance(2, k)
        count = 2 if k < half else 1

        def both_ways(q, carry, k=k):
            who = owner((place + n_sp - k + 2 * k * q) % n_sp)
            down(who)
            for c in down_copies(who):
                c.start()
            return carry

        lax.fori_loop(0, count, both_ways, 0)

    def settle(who, carry):
        for c in down_copies(who):
            c.wait()
        return carry

    lax.fori_loop(0, n_sp, settle, 0)
    channel = part[rows_of(mt), :].astype(f32)
    for d in range(1, n_tp):
        channel = channel + recv2[d].astype(f32)
    out_ref[...] = layer_norm(
        ALPHA * normed[mine, :].astype(f32) + channel, g2_ref[...]
    ).astype(bf16)

    for piece in range(3):
        for way in range(2):
            for s in range(hops[piece][way]):
                ring_copy(piece, way, s).wait_send()
    for c in rim_copies:
        c.wait_send()

    @pl.when(me + 1 < n_sp)
    def _():
        rim_norm.wait_send()

    for c in state_copies(0):
        c.wait_send()
    for d in range(1, half):

        @pl.when(me + 2 * d < n_sp)
        def _(d=d):
            for c in state_copies(d):
                c.wait_send()


def fused_shards(n_sp, n_tp, *args):
    (
        res, rv, xf, bf, cf, dt, doff, fade, elf, byp, xk, bk, ck, csv, mm, g1, v, w, s, vk, wk, g2
    ) = args
    f32, bf16 = jnp.float32, jnp.bfloat16
    rows, inner = xf.shape
    heads = dt.shape[1]
    width = mm.shape[1]
    ff = v.shape[1]
    row = lambda a: a.reshape(1, -1)
    half = n_sp // 2
    vmem = pl.BlockSpec(memory_space=pltpu.VMEM)
    hbm = pl.BlockSpec(memory_space=pl.ANY)
    dma = pltpu.SemaphoreType.DMA
    return pl.pallas_call(
        functools.partial(layer_kernel, n_sp, n_tp),
        out_shape=jax.ShapeDtypeStruct(res.shape, bf16),
        in_specs=[vmem] * 16 + [hbm] * 3 + [vmem] * 3,
        out_specs=vmem,
        scratch_shapes=[
            pltpu.VMEM((n_sp * v.shape[0], ff), bf16),
            pltpu.VMEM((n_sp * v.shape[0], ff), bf16),
            pltpu.VMEM((n_sp,) + s.shape, bf16),
            pltpu.VMEM((RIM, inner), bf16),
            pltpu.VMEM((RIM, STATE), bf16),
            pltpu.VMEM((RIM, STATE), bf16),
            pltpu.VMEM((rows + RIM, 128), f32),
            pltpu.VMEM((rows, inner), bf16),
            pltpu.VMEM((rows, STATE), bf16),
            pltpu.VMEM((rows, STATE), bf16),
            pltpu.VMEM((rows, heads), f32),
            pltpu.VMEM((rows, heads), f32),
            pltpu.VMEM((rows, inner), f32),
            pltpu.VMEM((rows, heads), f32),
            pltpu.VMEM((8, heads), f32),
            pltpu.VMEM((STATE, inner), f32),
            pltpu.VMEM((STATE, inner), bf16),
            pltpu.VMEM((8, heads), f32),
            pltpu.VMEM((STATE, inner), bf16),
            pltpu.VMEM((8, heads), f32),
            pltpu.VMEM((half, STATE, inner), bf16),
            pltpu.VMEM((half, 8, heads), f32),
            pltpu.VMEM((rows, width), bf16),
            pltpu.VMEM((n_tp, rows // n_tp, width), bf16),
            pltpu.VMEM((n_tp, rows // n_tp, width), bf16),
            pltpu.VMEM((rows + RIM, width), bf16),
            pltpu.VMEM((rows, ff), bf16),
            dma((3,)),
            dma((2, half, 3)),
            dma((2, half, 3)),
            dma((3,)),
            dma((3,)),
            dma((half, 2)),
            dma((half, 2)),
            dma((n_tp,)),
            dma((n_tp,)),
            dma((n_tp,)),
            dma((n_tp,)),
            dma((n_tp, n_sp)),
            dma((n_tp, n_sp)),
            dma,
            dma,
        ],
        compiler_params=pltpu.CompilerParams(
            collective_id=0, has_side_effects=True, vmem_limit_bytes=60 * 1024 * 1024
        ),
    )(
        res, rv, xf, bf, cf, dt, row(doff), row(fade), elf, row(byp), xk, bk, ck, row(csv), mm,
        row(g1), v, w, s, vk, wk, row(g2),
    )


def shards_for(n_sp, n_tp):
    def shards(*args):
        rows = args[2].shape[0]
        fits = (
            args[3].shape[1] == STATE
            and args[18].shape[1] % 128 == 0
            and args[16].shape[0] % 16 == 0
            and args[16].shape[1] % 128 == 0
            and n_sp % 2 == 0
            and n_sp >= 4
            and args[18].shape[0] % 32 == 0
            and rows % (BLOCK * n_tp) == 0
        )
        if fits:
            return fused_shards(n_sp, n_tp, *args)
        return plain_shards(*args)

    return shards


def solution(mesh):
    in_specs = (
        P(("sp", "tp"), None),
        P("sp", "tp"),
        P("sp", "tp"),
        P("sp", "tp"),
        P("sp", "tp"),
        P("sp", "tp"),
        P("tp"),
        P("tp"),
        P("sp", "tp"),
        P("tp"),
        P(None, "tp"),
        P(None, "tp"),
        P(None, "tp"),
        P("tp"),
        P("tp", None),
        P(),
        P("sp", "tp"),
        P("sp", "tp"),
        P("tp", "sp"),
        P(None, "tp"),
        P(None, "tp"),
        P(),
    )
    out_specs = P(("sp", "tp"), None)
    shards = shards_for(mesh.shape["sp"], mesh.shape["tp"])
    return jax.shard_map(shards, mesh=mesh, in_specs=in_specs, out_specs=out_specs, check_vma=False)
```

```python
import functools
import jax
import jax.numpy as jnp
from jax import lax
from jax.experimental import pallas as pl
from jax.experimental.pallas import tpu as pltpu
from jax.sharding import PartitionSpec as P

HEADS = 32
HEAD_DIM = 64
GROUPS = 4
STATE = 128
CONV = 4
FCONV = 3
BLOCK = 128


EPSILON = 1e-05
ALPHA = 2.0**0.25
HIGHEST = lax.Precision.HIGHEST


def shifted(shard, axis, by):
    count = lax.axis_size(axis)
    pairs = [(i, i + by) for i in range(count) if 0 <= i + by < count]
    return lax.ppermute(shard, axis, pairs)


def entering(shard, axis, join, neutral):
    place = lax.axis_index(axis)
    gathered = jax.tree.map(
        lambda a, kind: lax.all_gather(a.astype(kind), axis), shard, (jnp.bfloat16, jnp.bfloat16)
    )
    state = jax.tree.map(lambda a, e: jnp.zeros_like(a) + jnp.asarray(e, a.dtype), shard, neutral)

    def one(lap, state):
        return join(
            state,
            jax.tree.map(
                lambda a, own: lax.dynamic_index_in_dim(a, lap, 0, False).astype(own.dtype),
                gathered,
                shard,
            ),
        )

    return lax.fori_loop(0, place, one, state)


def causal_conv(signal, before, tap_weights):
    tap_count = tap_weights.shape[0]
    row_count = signal.shape[0]
    padded = jnp.concatenate([before, signal], axis=0).astype(jnp.float32)
    running = jnp.zeros(signal.shape, jnp.float32)
    for tap_index in range(tap_count):
        running = (
            running
            + tap_weights[tap_index].astype(jnp.float32) * padded[tap_index : tap_index + row_count]
        )
    return running


def layer_norm(values, scales):
    row_mean = jnp.mean(values, axis=-1, keepdims=True)
    centred = values - row_mean
    spread = jnp.mean(centred * centred, axis=-1, keepdims=True)
    return centred * lax.rsqrt(spread + EPSILON) * scales


def combine_states(earlier_pair, later_pair):
    return (
        earlier_pair[0] * later_pair[1][..., None, None] + later_pair[0],
        earlier_pair[1] * later_pair[1],
    )


def chain_step(state_now, inputs):
    fresh_one, decay_one = inputs
    return (state_now * decay_one[..., None, None] + fresh_one, state_now)


def plain_shards(
    incoming_residual_stream,
    result_valve,
    channel_feed_matrix,
    memory_feed_matrix,
    memory_query_matrix,
    unsoftened_deltas,
    delta_offset,
    channel_fading_speed,
    extra_log_fading,
    bypass_factor,
    channel_feed_kernel,
    memory_feed_kernel,
    memory_query_kernel,
    cluster_scaling_vector,
    mixer_result_matrix,
    initial_scaling_vector,
    valve_matrix,
    widen_matrix,
    shrink_matrix,
    valve_filter_kernel,
    widen_filter_kernel,
    latter_scaling_vector,
):
    row_count = channel_feed_matrix.shape[0]
    inner_here = channel_feed_matrix.shape[1]
    group_count = memory_feed_matrix.shape[1] // STATE
    group_heads = HEADS // GROUPS
    block_count = row_count // BLOCK
    rim_rows = CONV - 1
    rim_x, rim_b, rim_c = shifted(
        (
            channel_feed_matrix[row_count - rim_rows :],
            memory_feed_matrix[row_count - rim_rows :],
            memory_query_matrix[row_count - rim_rows :],
        ),
        "sp",
        1,
    )
    x_act = jax.nn.silu(causal_conv(channel_feed_matrix, rim_x, channel_feed_kernel)).astype(
        jnp.bfloat16
    )
    b_act = jax.nn.silu(causal_conv(memory_feed_matrix, rim_b, memory_feed_kernel)).astype(
        jnp.bfloat16
    )
    c_act = jax.nn.silu(causal_conv(memory_query_matrix, rim_c, memory_query_kernel)).astype(
        jnp.bfloat16
    )
    channel_delta_amount = jax.nn.softplus(unsoftened_deltas + delta_offset[None, :])
    log_fading_amount = extra_log_fading - channel_fading_speed[None, :] * channel_delta_amount
    x_heads = x_act.astype(jnp.float32).reshape(row_count, group_count, group_heads, HEAD_DIM)
    x_scaled = (
        x_heads * channel_delta_amount.reshape(row_count, group_count, group_heads)[..., None]
    )
    b_full = b_act.astype(jnp.float32).reshape(row_count, group_count, STATE)
    c_full = c_act.astype(jnp.float32).reshape(row_count, group_count, STATE)
    decay_full = log_fading_amount.reshape(row_count, group_count, group_heads)
    x_blk = x_scaled.reshape(block_count, BLOCK, group_count, group_heads, HEAD_DIM)
    b_blk = b_full.reshape(block_count, BLOCK, group_count, STATE)
    c_blk = c_full.reshape(block_count, BLOCK, group_count, STATE)
    b_narrow = b_act.reshape(block_count, BLOCK, group_count, STATE)
    c_narrow = c_act.reshape(block_count, BLOCK, group_count, STATE)
    decay_blk = decay_full.reshape(block_count, BLOCK, group_count, group_heads)
    cum_decay = jnp.cumsum(decay_blk, axis=1)
    causal = jnp.tril(jnp.ones((BLOCK, BLOCK), dtype=bool))
    between = cum_decay[:, :, None] - cum_decay[:, None, :]
    lag = jnp.exp(jnp.where(causal[None, :, :, None, None], between, -jnp.inf))
    affinity = jnp.einsum("blgn,bsgn->blsg", c_narrow, b_narrow, preferred_element_type=jnp.float32)
    mixing = affinity[..., None] * lag
    within = jnp.einsum("blsgh,bsghp->blghp", mixing, x_blk, precision=HIGHEST)
    to_end = jnp.exp(cum_decay[:, -1:] - cum_decay)
    fresh = jnp.einsum("blgn,blghp->bghpn", b_blk, x_blk * to_end[..., None], precision=HIGHEST)
    block_decay = jnp.exp(cum_decay[:, -1])
    initial = jnp.zeros((group_count, group_heads, HEAD_DIM, STATE), jnp.float32)
    local_end, earlier = lax.scan(chain_step, initial, (fresh, block_decay))
    carried = (
        jnp.einsum("blgn,bghpn->blghp", c_blk, earlier, precision=HIGHEST)
        * jnp.exp(cum_decay)[..., None]
    )
    from_start = jnp.cumsum(decay_full, axis=0)
    incoming, _ = entering(
        (local_end, jnp.exp(from_start[-1])),
        "sp",
        combine_states,
        (jnp.zeros_like(local_end), jnp.ones_like(from_start[-1])),
    )
    arriving = (
        jnp.einsum("tgn,ghpn->tghp", c_full, incoming, precision=HIGHEST)
        * jnp.exp(from_start)[..., None]
    )
    y_heads = (within + carried).reshape(row_count, group_count, group_heads, HEAD_DIM) + arriving
    y_heads = y_heads + bypass_factor.reshape(group_count, group_heads)[None, :, :, None] * x_heads
    gated = y_heads.reshape(row_count, group_count, group_heads * HEAD_DIM)
    gated = gated * jax.nn.silu(result_valve.astype(jnp.float32)).reshape(
        row_count, group_count, group_heads * HEAD_DIM
    )
    gated = gated * lax.rsqrt(jnp.mean(gated * gated, axis=-1, keepdims=True) + EPSILON)
    y_norm = (gated.reshape(row_count, inner_here) * cluster_scaling_vector[None, :]).astype(
        jnp.bfloat16
    )
    mixer = lax.psum_scatter(
        jnp.dot(y_norm, mixer_result_matrix, preferred_element_type=jnp.float32).astype(
            jnp.bfloat16
        ),
        "tp",
        scatter_dimension=0,
        tiled=True,
    ).astype(jnp.float32)
    normed_own = layer_norm(
        ALPHA * incoming_residual_stream.astype(jnp.float32) + mixer, initial_scaling_vector
    ).astype(jnp.bfloat16)
    normed_all = lax.all_gather(normed_own, "tp", axis=0, tiled=True)
    gate_sum = jnp.dot(
        normed_all,
        lax.all_gather(valve_matrix, "sp", axis=0, tiled=True),
        preferred_element_type=jnp.float32,
    )
    up_sum = jnp.dot(
        normed_all,
        lax.all_gather(widen_matrix, "sp", axis=0, tiled=True),
        preferred_element_type=jnp.float32,
    )
    gate_proj = gate_sum.astype(jnp.bfloat16)
    up_proj = up_sum.astype(jnp.bfloat16)
    ffn_rows = FCONV - 1
    rim_gate, rim_up = shifted(
        (gate_proj[row_count - ffn_rows :], up_proj[row_count - ffn_rows :]), "sp", 1
    )
    gate_conv = causal_conv(gate_proj, rim_gate, valve_filter_kernel)
    up_conv = causal_conv(up_proj, rim_up, widen_filter_kernel)
    hidden = (jax.nn.silu(gate_conv) * up_conv).astype(jnp.bfloat16)
    channel_part = jnp.dot(
        hidden,
        lax.all_gather(shrink_matrix, "sp", axis=1, tiled=True),
        preferred_element_type=jnp.float32,
    )
    channel = lax.psum_scatter(
        channel_part.astype(jnp.bfloat16), "tp", scatter_dimension=0, tiled=True
    ).astype(jnp.float32)
    return layer_norm(
        ALPHA * normed_own.astype(jnp.float32) + channel, latter_scaling_vector
    ).astype(jnp.bfloat16)


MESH = pl.DeviceIdType.MESH
RIM = 16


def silu(v):
    return v / (1.0 + jnp.exp(-v))


def layer_kernel(
    n_sp,
    n_tp,
    res_hbm,
    rv_hbm,
    xf_ref,
    bf_ref,
    cf_ref,
    dt_ref,
    doff_ref,
    fade_ref,
    elf_ref,
    byp_ref,
    xk_ref,
    bk_ref,
    ck_ref,
    csv_ref,
    mm_hbm,
    g1_ref,
    v_hbm,
    w_hbm,
    s_hbm,
    vk_ref,
    wk_ref,
    g2_ref,
    out_ref,
    v_all,
    w_all,
    s_all,
    rim_x,
    rim_b,
    rim_c,
    ext,
    x_act,
    b_act,
    c_act,
    step_ref,
    ld_ref,
    y_ref,
    efs_ref,
    base_ref,
    state_ref,
    st_send,
    dec_send,
    pair_send,
    pair_dec,
    st_recv,
    dec_recv,
    part,
    recv1,
    recv2,
    normed,
    hidden,
    res_ref,
    rv_ref,
    mm_ref,
    late_sem,
    own_sem,
    ring_send,
    ring_recv,
    rim_send,
    rim_recv,
    st_ssem,
    st_rsem,
    t1_send,
    t1_recv,
    t2_send,
    t2_recv,
    t3_send,
    t3_recv,
    nr_send,
    nr_recv,
):
    f32, bf16 = jnp.float32, jnp.bfloat16
    rows, inner = xf_ref.shape
    heads = dt_ref.shape[0]
    own_rows = rows // n_tp
    width = mm_hbm.shape[1]
    ff = v_hbm.shape[1]
    depth = v_hbm.shape[0]
    cols = s_hbm.shape[1]
    blocks = rows // BLOCK
    me = lax.axis_index("sp")
    mt = lax.axis_index("tp")
    half = n_sp // 2

    def owner(pos):
        back = pos // half
        return (1 - back) * 2 * pos + back * (2 * (n_sp - 1 - pos) + 1)

    odd = me % 2
    place = (1 - odd) * (me // 2) + odd * (n_sp - 1 - me // 2)
    after = owner((place + 1) % n_sp)
    ahead = owner((place + n_sp - 1) % n_sp)

    barrier = pltpu.get_barrier_semaphore()
    for d in range(1, n_sp):
        pl.semaphore_signal(barrier, inc=1, device_id=((me + d) % n_sp, mt), device_id_type=MESH)
    for d in range(1, n_tp):
        pl.semaphore_signal(barrier, inc=1, device_id=(me, (mt + d) % n_tp), device_id_type=MESH)
    pl.semaphore_wait(barrier, n_sp + n_tp - 2)

    def slot(piece, who):
        if piece == 2:
            return s_all.at[who]
        whole = v_all if piece == 0 else w_all
        return whole.at[pl.ds(pl.multiple_of(who * depth, depth), depth)]

    sources = (v_hbm, w_hbm, s_hbm)
    hops = {}
    for piece in range(3):
        long_way = half if piece != 1 else n_sp - 1 - half
        hops[piece] = (long_way, n_sp - 1 - long_way) if piece < 2 else (half, half)

    def ring_copy(piece, way, step):
        who = owner((place + n_sp - step) % n_sp if way == 0 else (place + step) % n_sp)
        src = sources[piece] if step == 0 else slot(piece, who)
        dst = slot(piece, who)
        if piece == 2 and step == half - 1:
            part_rows = src.shape[0] // 2
            here = pl.ds(way * part_rows, part_rows)
            src, dst = src.at[here], dst.at[here]
        return pltpu.make_async_remote_copy(
            src_ref=src,
            dst_ref=dst,
            send_sem=ring_send.at[way, step, piece],
            recv_sem=ring_recv.at[way, step, piece],
            device_id=(after if way == 0 else ahead, mt),
            device_id_type=MESH,
        )

    def advance(piece, step):
        for way in range(2):
            if 1 <= step <= hops[piece][way]:
                ring_copy(piece, way, step - 1).wait_recv()
            if step < hops[piece][way]:
                ring_copy(piece, way, step).start()

    rim_copies = []
    for i, (a, b) in enumerate(((xf_ref, rim_x), (bf_ref, rim_b), (cf_ref, rim_c))):
        rim_copies.append(
            pltpu.make_async_remote_copy(
                src_ref=a.at[pl.ds(rows - RIM, RIM)],
                dst_ref=b,
                send_sem=rim_send.at[i],
                recv_sem=rim_recv.at[i],
                device_id=((me + 1) % n_sp, mt),
                device_id_type=MESH,
            )
        )
        rim_copies[-1].start()
    own_copies = []
    for piece in range(3):
        if piece < 2:
            advance(piece, 0)
        own_copies.append(
            pltpu.make_async_copy(sources[piece], slot(piece, me), own_sem.at[piece])
        )
        own_copies[-1].start()

    late = [
        pltpu.make_async_copy(a, b, late_sem.at[i])
        for i, (a, b) in enumerate(((rv_hbm, rv_ref), (mm_hbm, mm_ref), (res_hbm, res_ref)))
    ]
    for c in late:
        c.start()

    eye = lax.broadcasted_iota(jnp.int32, (heads, heads), 0) == lax.broadcasted_iota(
        jnp.int32, (heads, heads), 1
    )

    def column(a):
        return jnp.sum(jnp.where(eye, a[...], 0.0), axis=1, keepdims=True)

    raw = dt_ref[...] + column(doff_ref)
    step_ref[...] = jnp.maximum(raw, 0.0) + jnp.log1p(jnp.exp(-jnp.abs(raw)))
    ld_ref[...] = elf_ref[...] - column(fade_ref) * step_ref[...]

    for c in rim_copies:
        c.wait_recv()
    first = me == 0
    for rim, feed, taps, act in (
        (rim_x, xf_ref, xk_ref, x_act),
        (rim_b, bf_ref, bk_ref, b_act),
        (rim_c, cf_ref, ck_ref, c_act),
    ):
        for lo in range(0, feed.shape[1], 128):
            here = slice(lo, lo + 128)
            edge = rim[:, here].astype(f32)
            ext[0:RIM, :] = jnp.where(first, jnp.zeros_like(edge), edge)
            ext[RIM:, :] = feed[:, here].astype(f32)
            tap = taps[:, here].astype(f32)
            total = jnp.zeros((rows, 128), f32)
            for k in range(CONV):
                start = RIM - (CONV - 1) + k
                total = total + tap[k : k + 1] * ext[start : start + rows, :]
            act[:, here] = silu(total).astype(bf16)

    li = lax.broadcasted_iota(jnp.int32, (BLOCK, BLOCK), 0)
    si = lax.broadcasted_iota(jnp.int32, (BLOCK, BLOCK), 1)
    causal = li >= si
    lower = jnp.where(causal, 1.0, 0.0).astype(f32)
    upper = jnp.where(li <= si, 1.0, 0.0).astype(f32)
    spread = jnp.where(
        lax.broadcasted_iota(jnp.int32, (heads, inner), 1) // HEAD_DIM
        == lax.broadcasted_iota(jnp.int32, (heads, inner), 0),
        1.0,
        0.0,
    ).astype(f32)
    near = lax.broadcasted_iota(jnp.int32, (BLOCK, 2 * HEAD_DIM), 1) < HEAD_DIM

    def widen(a):
        return jnp.dot(a, spread, precision=HIGHEST, preferred_element_type=f32)

    state_ref[...] = jnp.zeros_like(state_ref)
    base_ref[...] = jnp.zeros_like(base_ref)
    skip = widen(byp_ref[...])

    def scan_block(b, carry):
        at = pl.ds(pl.multiple_of(b * BLOCK, BLOCK), BLOCK)
        ld = ld_ref[:, at]
        cum = lax.dot_general(
            lower, ld, (((1,), (1,)), ((), ())), precision=HIGHEST, preferred_element_type=f32
        )
        cum_t = jnp.dot(ld, upper, precision=HIGHEST, preferred_element_type=f32)
        last = cum[BLOCK - 1 : BLOCK, :]
        x = x_act[at, :].astype(f32)
        bb = b_act[at, :]
        cc = c_act[at, :]
        xs = x * lax.dot_general(
            step_ref[:, at],
            spread,
            (((0,), (0,)), ((), ())),
            precision=HIGHEST,
            preferred_element_type=f32,
        )
        xs16 = xs.astype(bf16)
        aff = lax.dot_general(
            cc, bb, (((1,), (1,)), ((), ())), preferred_element_type=f32
        )
        y = (
            jnp.dot(cc, state_ref[...].astype(bf16), preferred_element_type=f32)
            * widen(jnp.exp(cum))
            + skip * x
        )
        for pair in range(heads // 2):
            at_pair = slice(pair * 2 * HEAD_DIM, (pair + 1) * 2 * HEAD_DIM)
            both = []
            for h in (2 * pair, 2 * pair + 1):
                gap = cum[:, h : h + 1] - cum_t[h : h + 1, :]
                lag = jnp.exp(jnp.where(causal, gap, -1e30))
                both.append(
                    jnp.dot(
                        (aff * lag).astype(bf16), xs16[:, at_pair], preferred_element_type=f32
                    )
                )
            y_ref[at, at_pair] = y[:, at_pair] + jnp.where(near, both[0], both[1])
        fresh = lax.dot_general(
            bb,
            (xs * widen(jnp.exp(last - cum))).astype(bf16),
            (((0,), (0,)), ((), ())),
            preferred_element_type=f32,
        )
        state_ref[...] = state_ref[...] * widen(jnp.exp(last)) + fresh
        base = base_ref[0:1, :]
        efs_ref[at, :] = jnp.exp(base + cum)
        base_ref[0:1, :] = base + last
        return carry

    lax.fori_loop(0, blocks, scan_block, 0)
    st_send[...] = state_ref[...].astype(bf16)
    dec_send[...] = jnp.broadcast_to(base_ref[0:1, :], dec_send.shape)
    partner = me + 1 - 2 * odd

    def state_copies(d):
        pair = d > 0
        return [
            pltpu.make_async_remote_copy(
                src_ref=a,
                dst_ref=b.at[d],
                send_sem=st_ssem.at[d, i],
                recv_sem=st_rsem.at[d, i],
                device_id=((me + 2 * d) % n_sp if pair else partner, mt),
                device_id_type=MESH,
            )
            for i, (a, b) in enumerate(
                ((pair_send if pair else st_send, st_recv), (pair_dec if pair else dec_send, dec_recv))
            )
        ]

    for c in state_copies(0):
        c.start()
    advance(0, 1)
    for c in state_copies(0):
        c.wait_recv()
    own_dec = widen(jnp.exp(dec_send[0:1, :]))
    beside_dec = widen(jnp.exp(dec_recv[0, 0:1, :]))
    beside = st_recv[0].astype(f32)
    later = odd == 1
    pair_send[...] = jnp.where(
        later, state_ref[...] + beside * own_dec, state_ref[...] * beside_dec + beside
    ).astype(bf16)
    pair_dec[...] = dec_send[...] + dec_recv[0]
    state_ref[...] = jnp.zeros_like(state_ref)
    for d in range(1, half):

        @pl.when(me + 2 * d < n_sp)
        def _(d=d):
            for c in state_copies(d):
                c.start()

    advance(1, 1)
    advance(2, 0)
    for d in range(half - 1, 0, -1):

        @pl.when(me >= 2 * d)
        def _(d=d):
            for c in state_copies(d):
                c.wait_recv()
            state_ref[...] = state_ref[...] * widen(
                jnp.exp(dec_recv[d, 0:1, :])
            ) + st_recv[d].astype(f32)

    @pl.when(odd == 1)
    def _():
        state_ref[...] = state_ref[...] * widen(jnp.exp(dec_recv[0, 0:1, :])) + st_recv[
            0
        ].astype(f32)

    for c in late:
        c.wait()

    def project_block(b, carry):
        at = pl.ds(pl.multiple_of(b * BLOCK, BLOCK), BLOCK)
        y = y_ref[at, :] + jnp.dot(
            c_act[at, :], state_ref[...].astype(bf16), preferred_element_type=f32
        ) * widen(efs_ref[at, :])
        gated = y * silu(rv_ref[at, :].astype(f32))
        gated = gated * lax.rsqrt(jnp.mean(gated * gated, axis=-1, keepdims=True) + EPSILON)
        y_norm = (gated * csv_ref[...]).astype(bf16)
        part[at, :] = jnp.dot(y_norm, mm_ref[...], preferred_element_type=f32).astype(bf16)
        return carry

    lax.fori_loop(0, blocks, project_block, 0)

    def rows_of(t):
        return pl.ds(pl.multiple_of(t * own_rows, own_rows), own_rows)

    def tp_copy(d, src, dst, send, recv):
        return pltpu.make_async_remote_copy(
            src_ref=src,
            dst_ref=dst,
            send_sem=send,
            recv_sem=recv,
            device_id=(me, (mt + d) % n_tp),
            device_id_type=MESH,
        )

    first_sum = [
        tp_copy(d, part.at[rows_of((mt + d) % n_tp)], recv1.at[d], t1_send.at[d], t1_recv.at[d])
        for d in range(1, n_tp)
    ]
    for c in first_sum:
        c.start()
    advance(0, 2)
    for c in first_sum:
        c.wait_recv()
    mixer = part[rows_of(mt), :].astype(f32)
    for d in range(1, n_tp):
        mixer = mixer + recv1[d].astype(f32)
    mine = pl.ds(pl.multiple_of(RIM + mt * own_rows, RIM), own_rows)
    normed[mine, :] = layer_norm(
        ALPHA * res_ref[...].astype(f32) + mixer, g1_ref[...]
    ).astype(bf16)
    for c in first_sum:
        c.wait_send()
    spread_rows = [
        tp_copy(d, normed.at[mine], normed.at[mine], t2_send.at[d], t2_recv.at[d])
        for d in range(1, n_tp)
    ]
    for c in spread_rows:
        c.start()
    advance(1, 2)
    advance(0, 3)
    for c in spread_rows:
        c.wait()
    rim_norm = pltpu.make_async_remote_copy(
        src_ref=normed.at[pl.ds(rows, RIM)],
        dst_ref=normed.at[pl.ds(0, RIM)],
        send_sem=nr_send,
        recv_sem=nr_recv,
        device_id=((me + 1) % n_sp, mt),
        device_id_type=MESH,
    )

    @pl.when(me + 1 < n_sp)
    def _():
        rim_norm.start()

    @pl.when(me == 0)
    def _():
        normed[0:RIM, :] = jnp.zeros((RIM, width), bf16)

    advance(1, 3)
    advance(2, 1)
    for s in range(4, half + 1):
        advance(0, s)
        advance(1, s)

    @pl.when(me > 0)
    def _():
        rim_norm.wait_recv()

    for c in own_copies:
        c.wait()

    def ffn_cols(at):
        feeds = normed[...]
        convs = []
        for weights, taps in ((v_all, vk_ref), (w_all, wk_ref)):
            proj = jnp.dot(feeds, weights[:, at], preferred_element_type=f32)
            proj = proj.astype(bf16).astype(f32)
            tap = taps[:, at].astype(f32)
            total = jnp.zeros((rows, proj.shape[1]), f32)
            for k in range(FCONV):
                start = RIM - (FCONV - 1) + k
                total = total + tap[k : k + 1] * proj[start : start + rows, :]
            convs.append(total)
        hidden[:, at] = (silu(convs[0]) * convs[1]).astype(bf16)

    chunk = 256
    full = ff // chunk

    def ffn_chunk(i, carry):
        ffn_cols(pl.ds(pl.multiple_of(i * chunk, chunk), chunk))
        return carry

    lax.fori_loop(0, full // 2, ffn_chunk, 0)
    advance(2, 2)
    lax.fori_loop(full // 2, full, ffn_chunk, 0)
    if ff % chunk:
        ffn_cols(pl.ds(full * chunk, ff % chunk))

    def down(who):
        at = pl.ds(pl.multiple_of(who * cols, cols), cols)
        part[:, at] = jnp.dot(
            hidden[...], s_all[who], preferred_element_type=f32
        ).astype(bf16)

    def down_copies(who):
        at = pl.ds(pl.multiple_of(who * cols, cols), cols)
        return [
            tp_copy(
                d,
                part.at[rows_of((mt + d) % n_tp), at],
                recv2.at[d, :, at],
                t3_send.at[d, who],
                t3_recv.at[d, who],
            )
            for d in range(1, n_tp)
        ]

    down(me)
    for c in down_copies(me):
        c.start()
    for k in range(1, half + 1):
        if k >= 3:
            advance(2, k)
        count = 2 if k < half else 1

        def both_ways(q, carry, k=k):
            who = owner((place + n_sp - k + 2 * k * q) % n_sp)
            down(who)
            for c in down_copies(who):
                c.start()
            return carry

        lax.fori_loop(0, count, both_ways, 0)

    def settle(who, carry):
        for c in down_copies(who):
            c.wait()
        return carry

    lax.fori_loop(0, n_sp, settle, 0)
    channel = part[rows_of(mt), :].astype(f32)
    for d in range(1, n_tp):
        channel = channel + recv2[d].astype(f32)
    out_ref[...] = layer_norm(
        ALPHA * normed[mine, :].astype(f32) + channel, g2_ref[...]
    ).astype(bf16)

    for piece in range(3):
        for way in range(2):
            for s in range(hops[piece][way]):
                ring_copy(piece, way, s).wait_send()
    for c in rim_copies:
        c.wait_send()

    @pl.when(me + 1 < n_sp)
    def _():
        rim_norm.wait_send()

    for c in state_copies(0):
        c.wait_send()
    for d in range(1, half):

        @pl.when(me + 2 * d < n_sp)
        def _(d=d):
            for c in state_copies(d):
                c.wait_send()


def fused_shards(n_sp, n_tp, *args):
    (
        res, rv, xf, bf, cf, dt, doff, fade, elf, byp, xk, bk, ck, csv, mm, g1, v, w, s, vk, wk, g2
    ) = args
    f32, bf16 = jnp.float32, jnp.bfloat16
    rows, inner = xf.shape
    heads = dt.shape[1]
    width = mm.shape[1]
    ff = v.shape[1]
    row = lambda a: a.reshape(1, -1)
    half = n_sp // 2
    vmem = pl.BlockSpec(memory_space=pltpu.VMEM)
    hbm = pl.BlockSpec(memory_space=pl.ANY)
    dma = pltpu.SemaphoreType.DMA
    return pl.pallas_call(
        functools.partial(layer_kernel, n_sp, n_tp),
        out_shape=jax.ShapeDtypeStruct(res.shape, bf16),
        in_specs=[hbm] * 2 + [vmem] * 12 + [hbm, vmem] + [hbm] * 3 + [vmem] * 3,
        out_specs=vmem,
        scratch_shapes=[
            pltpu.VMEM((n_sp * v.shape[0], ff), bf16),
            pltpu.VMEM((n_sp * v.shape[0], ff), bf16),
            pltpu.VMEM((n_sp,) + s.shape, bf16),
            pltpu.VMEM((RIM, inner), bf16),
            pltpu.VMEM((RIM, STATE), bf16),
            pltpu.VMEM((RIM, STATE), bf16),
            pltpu.VMEM((rows + RIM, 128), f32),
            pltpu.VMEM((rows, inner), bf16),
            pltpu.VMEM((rows, STATE), bf16),
            pltpu.VMEM((rows, STATE), bf16),
            pltpu.VMEM((heads, rows), f32),
            pltpu.VMEM((heads, rows), f32),
            pltpu.VMEM((rows, inner), f32),
            pltpu.VMEM((rows, heads), f32),
            pltpu.VMEM((8, heads), f32),
            pltpu.VMEM((STATE, inner), f32),
            pltpu.VMEM((STATE, inner), bf16),
            pltpu.VMEM((8, heads), f32),
            pltpu.VMEM((STATE, inner), bf16),
            pltpu.VMEM((8, heads), f32),
            pltpu.VMEM((half, STATE, inner), bf16),
            pltpu.VMEM((half, 8, heads), f32),
            pltpu.VMEM((rows, width), bf16),
            pltpu.VMEM((n_tp, rows // n_tp, width), bf16),
            pltpu.VMEM((n_tp, rows // n_tp, width), bf16),
            pltpu.VMEM((rows + RIM, width), bf16),
            pltpu.VMEM((rows, ff), bf16),
            pltpu.VMEM(res.shape, bf16),
            pltpu.VMEM(rv.shape, bf16),
            pltpu.VMEM(mm.shape, bf16),
            dma((3,)),
            dma((3,)),
            dma((2, half, 3)),
            dma((2, half, 3)),
            dma((3,)),
            dma((3,)),
            dma((half, 2)),
            dma((half, 2)),
            dma((n_tp,)),
            dma((n_tp,)),
            dma((n_tp,)),
            dma((n_tp,)),
            dma((n_tp, n_sp)),
            dma((n_tp, n_sp)),
            dma,
            dma,
        ],
        compiler_params=pltpu.CompilerParams(
            collective_id=0, has_side_effects=True, vmem_limit_bytes=60 * 1024 * 1024
        ),
    )(
        res, rv, xf, bf, cf, dt.T, row(doff), row(fade), elf.T, row(byp), xk, bk, ck, row(csv), mm,
        row(g1), v, w, s, vk, wk, row(g2),
    )


def shards_for(n_sp, n_tp):
    def shards(*args):
        rows = args[2].shape[0]
        fits = (
            args[3].shape[1] == STATE
            and args[18].shape[1] % 128 == 0
            and args[16].shape[0] % 16 == 0
            and args[16].shape[1] % 128 == 0
            and n_sp % 2 == 0
            and n_sp >= 4
            and args[18].shape[0] % 32 == 0
            and rows % (BLOCK * n_tp) == 0
        )
        if fits:
            return fused_shards(n_sp, n_tp, *args)
        return plain_shards(*args)

    return shards


def solution(mesh):
    in_specs = (
        P(("sp", "tp"), None),
        P("sp", "tp"),
        P("sp", "tp"),
        P("sp", "tp"),
        P("sp", "tp"),
        P("sp", "tp"),
        P("tp"),
        P("tp"),
        P("sp", "tp"),
        P("tp"),
        P(None, "tp"),
        P(None, "tp"),
        P(None, "tp"),
        P("tp"),
        P("tp", None),
        P(),
        P("sp", "tp"),
        P("sp", "tp"),
        P("tp", "sp"),
        P(None, "tp"),
        P(None, "tp"),
        P(),
    )
    out_specs = P(("sp", "tp"), None)
    shards = shards_for(mesh.shape["sp"], mesh.shape["tp"])
    return jax.shard_map(shards, mesh=mesh, in_specs=in_specs, out_specs=out_specs, check_vma=False)
```
